32 devices in a mesh: sp: 4 (over y, x), tp: 8 (over z, core).
Axes of the slice: x: 2, y: 2, z: 4, core: 2. Of those that a mesh axis runs over, the one named last changes fastest.
Arguments:
- queries: bfloat16 [1536, 2048], P('sp', 'tp'), may hold values from -6 to 6
- keys: bfloat16 [1536, 2048], P('sp', 'tp'), may hold values from -6 to 6
- values: bfloat16 [1536, 2048], P('sp', 'tp'), may hold values from -6 to 6
- key_bias: bfloat16 [1536, 32], P('sp', 'tp'), may hold values from -16 to 0
- head_gain: float32 [32, 64], P('tp'), may hold values from 0.1 to 1.9
- out_weight: bfloat16 [2048, 2048], P('tp'), may hold values from -0.125 to 0.125
- residual: bfloat16 [1536, 2048], P(('sp', 'tp')), may hold values from -6 to 6
- norm_gain: float32 [2048], replicated, may hold values from 0.1 to 1.9
- gate_proj: bfloat16 [4, 2048, 7168], P('sp', None, 'tp'), may hold values from -0.125 to 0.125
- up_proj: bfloat16 [4, 2048, 7168], P('sp', None, 'tp'), may hold values from -0.125 to 0.125
- down_proj: bfloat16 [4, 7168, 2048], P('sp', 'tp'), may hold values from -0.0625 to 0.0625
- expert_choice: int32 [1536, 2], P(('sp', 'tp')), may hold values from 0 to 3, all different within a row; in each aligned block of 48 rows (0 to 47, 48 to 95, ...) at most 48 rows name the same one
- expert_weights: float32 [1536, 2], P(('sp', 'tp')), may hold values from 0.2 to 1
Outputs:
- layer_out: bfloat16 [1536, 2048], P(('sp', 'tp'))
The draws below stay inside these ranges and needn't reach their ends.
Inputs may be any that keep to these rules, and one draw needn't show every extreme that they name: `expert_choice`: in each aligned block of 48 rows (the rows of one device), no expert is named more than 48 times; the two experts of a row differ.
All inputs are finite; a program needn't handle non-finite values.
Results may differ from the reference program's by a relative error of at most 0.019.
Values may be sent and summed in bfloat16 or wider, within the bound.
A program may use at most 128 MiB of HBM per device.

```python
import math
import jax
import jax.numpy as jnp
import numpy as np
from jax import lax

D = 2048
HEADS = 32
HEAD_DIM = 64
FFE = 7168
TOK_DEV = 384
TOKENS = 1536
EXPERTS = 4
ROWS_DEV = 48
CAP = 48
N_TP = 8


def draw_key_bias(key, part):
    streams = jax.random.split(jax.random.fold_in(key, 11), 7)
    chance = 0.5
    slow_heads = jax.random.uniform(streams[0], (HEADS,)) < chance
    fast_base = jax.random.uniform(streams[1], (HEADS,), minval=-5.0, maxval=-3.8)
    slow_base = -jnp.log(jnp.float32(TOKENS)) - 0.5 + jax.random.uniform(streams[2], (HEADS,), minval=-0.5, maxval=0.5)
    blocks = TOKENS // TOK_DEV
    device_factor = jax.random.uniform(streams[3], (blocks, 1, HEADS), minval=-0.7, maxval=0.7)
    device_factor = jnp.broadcast_to(device_factor, (blocks, TOK_DEV, HEADS)).reshape(TOKENS, HEADS)
    jitter = 0.3 * jax.random.normal(streams[4], (TOKENS, HEADS))
    base = jnp.where(slow_heads[None, :], slow_base[None, :], fast_base[None, :]) + device_factor + jitter
    spots = jax.random.randint(streams[5], (2,), 0, TOKENS)
    levels = jax.random.uniform(streams[6], (2, HEADS), minval=-1.4, maxval=0.0)
    position = jnp.arange(TOKENS)
    first_hit = (position == spots[0])[:, None] & slow_heads[None, :]
    second_hit = (position == spots[1])[:, None] & slow_heads[None, :]
    base = jnp.where(first_hit, levels[0][None, :], base)
    base = jnp.where(second_hit, levels[1][None, :], base)
    return jnp.clip(base, -16.0, 0.0).astype(jnp.bfloat16)


def block_levels(stream_key, extent, pieces, smallest, top_value):
    factor_of, own = 1.0, jax.random.fold_in(stream_key, 6)
    for dim, blocks in pieces:
        heights = jnp.exp(jax.random.uniform(jax.random.fold_in(own, dim), (blocks,), jnp.float32, smallest / len(pieces), top_value / len(pieces)))
        factor_of = factor_of * jnp.repeat(heights, extent[dim] // blocks).reshape([-1 if axis == dim else 1 for axis in range(len(extent))])
    return factor_of


def assign_block(key, own, number, rows, count, top, bound, skew):
    sequence = jax.random.permutation(key, count)
    heavy_load, ordinary = shares(count, rows * top, bound, skew, True), shares(count, rows * top, bound, skew, False)
    places = jnp.arange(count)

    def named(tallies, rotation):
        used = int((tallies > 0).sum())
        fixed = max(1, used // 4)
        shifted = fixed + (places - fixed + rotation * (used - fixed)) % max(1, count - fixed)
        return jnp.zeros((count,), jnp.int32).at[sequence[jnp.where(places < fixed, places, shifted)]].set(jnp.asarray(tallies, jnp.int32))

    tallies = jnp.where(number % 4 == 0, named(heavy_load, number // 4), named(ordinary, number - number // 4 - 1))
    mixed = jax.random.permutation(jax.random.fold_in(own, 3), count)
    giver, taker = mixed[0:count // 2 * 2:2], mixed[1:count // 2 * 2:2]
    margin = jnp.minimum(tallies[giver] - 1, bound - tallies[taker]) // 2
    margin = jnp.where((giver == sequence[0]) | (taker == sequence[0]) | (tallies[taker] == 0), 0, jnp.maximum(margin, 0))
    shifted = jax.random.randint(jax.random.fold_in(own, 4), (count // 2,), 0, 1 << 20) % (margin + 1)
    tallies = tallies.at[giver].add(-shifted).at[taker].add(shifted)
    items = jnp.searchsorted(jnp.cumsum(tallies), jnp.arange(rows * top), side="right").astype(jnp.int32)
    table = items.reshape(top, rows).T
    table = table[jax.random.permutation(jax.random.fold_in(own, 1), rows)]
    rotation = jax.random.randint(jax.random.fold_in(own, 2), (rows, 1), 0, top)
    return jnp.take_along_axis(table, (jnp.arange(top)[None, :] + rotation) % top, axis=1)


def shares(count, total, limit, slope, full):
    weights = [(1 << 20) // math.isqrt(standing ** slope) + 1 for standing in range(1, count + 1)]
    largest = limit if full else min(limit, max(-(-total // count), total * weights[0] // sum(weights)))
    least = 1 if total - largest >= count - 1 else 0
    counts, spare = [largest] + [least] * (count - 1), total - largest - least * (count - 1)
    while spare > 0:
        movable = [i for i in range(1, count) if counts[i] < largest] or [i for i in range(1, count) if counts[i] < limit]
        whole, remaining = sum([weights[i] for i in movable]), spare
        for i in movable:
            addition = min(limit - counts[i], max(1, remaining * weights[i] // whole), spare)
            counts[i] = counts[i] + addition
            spare = spare - addition
    return np.array(counts)


def scatter_about(key, shape, spread, reach, shards=(), held_as=jnp.bfloat16):
    gain = block_levels(key, shape, shards, -0.22, 0.18) if shards else 1.0
    values = jax.random.normal(key, shape, jnp.float32) * spread * gain
    return jnp.minimum(jnp.maximum(values, -reach), reach).astype(held_as)


def setup_inputs(seed: int = 0) -> dict:
    key_of = jax.random.split(jax.random.key(seed), 14)
    queries = scatter_about(key_of[0], (TOKENS, HEADS * HEAD_DIM), 1.0, 6.0, ((0, 4), (1, 8)))
    keys = scatter_about(key_of[1], (TOKENS, HEADS * HEAD_DIM), 1.0, 6.0, ((0, 4), (1, 8)))
    values = scatter_about(key_of[2], (TOKENS, HEADS * HEAD_DIM), 1.0, 6.0, ((0, 4), (1, 8)))
    key_bias = draw_key_bias(jax.random.fold_in(key_of[13], 71), 0)
    head_gain = jnp.clip(1.0 + 0.18 * jax.random.normal(key_of[4], (HEADS, HEAD_DIM), jnp.float32), 0.1, 1.9)
    out_weight = scatter_about(key_of[5], (HEADS * HEAD_DIM, D), (HEADS * HEAD_DIM) ** -0.5, 0.125, ((0, 8),))
    residual = scatter_about(key_of[6], (TOKENS, D), 1.0, 6.0, ((0, 32),))
    norm_gain = jnp.clip(1.0 + 0.18 * jax.random.normal(key_of[7], (D,), jnp.float32), 0.1, 1.9)
    gate_proj = scatter_about(key_of[8], (EXPERTS, D, FFE), D ** -0.5, 0.125, ((0, 4), (2, 8)))
    up_proj = scatter_about(key_of[9], (EXPERTS, D, FFE), D ** -0.5, 0.125, ((0, 4), (2, 8)))
    down_proj = scatter_about(key_of[10], (EXPERTS, FFE, D), FFE ** -0.5, 0.0625, ((0, 4), (1, 8)))
    expert_choice_keys = jax.random.split(jax.random.fold_in(key_of[11], 1), TOKENS // ROWS_DEV)
    expert_choice_turns = jax.random.permutation(jax.random.fold_in(key_of[11], 3), TOKENS // ROWS_DEV)
    expert_choice = jax.vmap(lambda own, number: assign_block(jax.random.fold_in(key_of[11], 2), own, number, ROWS_DEV, EXPERTS, 2, CAP, 1))(expert_choice_keys, expert_choice_turns).reshape((TOKENS, 2))
    expert_weights = jnp.clip(0.2 + 0.8 * jax.random.uniform(key_of[12], (TOKENS, 2), jnp.float32) ** block_levels(key_of[12], (TOKENS, 2), ((0, 32),), -0.2, 0.2), 0.2, 1.0)
    return {"queries": queries, "keys": keys, "values": values, "key_bias": key_bias, "head_gain": head_gain, "out_weight": out_weight, "residual": residual, "norm_gain": norm_gain, "gate_proj": gate_proj, "up_proj": up_proj, "down_proj": down_proj, "expert_choice": expert_choice, "expert_weights": expert_weights}


epsilon = 1e-06

def rms_scaled(values_in):
    return values_in * lax.rsqrt(lax.optimization_barrier(jnp.mean(values_in * values_in, axis=-1, keepdims=True)) + epsilon)

def head_mixture(operands):
    query_head, key_head, value_head, bias_head = operands
    length = query_head.shape[0]
    blocks = length // TOK_DEV
    scores = jnp.dot(query_head, key_head.T, preferred_element_type=jnp.float32) * HEAD_DIM ** (-0.5)
    scores = scores + bias_head.astype(jnp.float32)[None, :]
    position = jnp.arange(length, dtype=jnp.int32)
    earlier = (position[None, :] < position[:, None]).reshape(length, blocks, TOK_DEV)
    scores = scores.reshape(length, blocks, TOK_DEV)
    log_drops = jnp.where(earlier, jax.nn.log_sigmoid(-scores), 0.0)
    suffix = lax.cumsum(log_drops, axis=2, reverse=True) - log_drops
    within = jnp.where(earlier, jnp.exp(jax.nn.log_sigmoid(scores) + suffix), 0.0).astype(jnp.bfloat16)
    value_blocks = value_head.reshape(blocks, TOK_DEV, HEAD_DIM).astype(jnp.float32)
    block_sums = jnp.einsum('tms,msd->tmd', within.astype(jnp.float32), value_blocks)
    totals = lax.optimization_barrier(jnp.sum(log_drops, axis=2))
    carried = lax.optimization_barrier(jnp.sum(totals, axis=1, keepdims=True)) - jnp.cumsum(totals, axis=1)
    return lax.optimization_barrier(jnp.sum(jnp.exp(carried)[:, :, None] * block_sums, axis=1))

def reference(queries, keys, values, key_bias, head_gain, out_weight, residual, norm_gain, gate_proj, up_proj, down_proj, expert_choice, expert_weights):

    def split_heads(array):
        return array.reshape(TOKENS, HEADS, HEAD_DIM).transpose(1, 0, 2)
    mixture = lax.map(head_mixture, (split_heads(queries), split_heads(keys), split_heads(values), key_bias.T))
    attended = (rms_scaled(mixture) * head_gain[:, None, :]).astype(jnp.bfloat16)
    attended = attended.transpose(1, 0, 2).reshape(TOKENS, HEADS * HEAD_DIM)
    projected = jnp.dot(attended, out_weight, preferred_element_type=jnp.float32)
    stream = (residual.astype(jnp.float32) + projected).astype(jnp.bfloat16)
    normed = (rms_scaled(stream.astype(jnp.float32)) * norm_gain).astype(jnp.bfloat16)
    device_blocks = TOKENS // ROWS_DEV
    flat_expert = expert_choice.reshape(-1).astype(jnp.int32)
    flat_token = jnp.arange(2 * TOKENS, dtype=jnp.int32) // 2
    onehot = (flat_expert[:, None] == jnp.arange(EXPERTS, dtype=jnp.int32)[None, :]).astype(jnp.int32)
    grouped = onehot.reshape(device_blocks, 2 * ROWS_DEV, EXPERTS)
    before = (jnp.cumsum(grouped, axis=1) - grouped).reshape(2 * TOKENS, EXPERTS)
    slot_rank = lax.optimization_barrier(jnp.sum(before * onehot, axis=1)).astype(jnp.int32)
    slot_index = (flat_token // ROWS_DEV * CAP + slot_rank).astype(jnp.int32)
    slot_table = jnp.full((EXPERTS, device_blocks * CAP), TOKENS, jnp.int32).at[flat_expert, slot_index].set(flat_token)
    padded = jnp.concatenate([normed, jnp.zeros((1, D), jnp.bfloat16)], axis=0)
    group_size = FFE // N_TP

    def one_expert(operands):
        rows_index, gate_matrix, up_matrix, down_matrix = operands
        row_block = padded[rows_index]
        gate_part = jnp.dot(row_block, gate_matrix, preferred_element_type=jnp.float32)
        up_part = jnp.dot(row_block, up_matrix, preferred_element_type=jnp.float32)
        hidden = (jax.nn.silu(gate_part) * up_part).astype(jnp.bfloat16)
        hidden_groups = hidden.reshape(row_block.shape[0], N_TP, group_size).transpose(1, 0, 2)
        down_groups = down_matrix.reshape(N_TP, group_size, D)

        def add_group(running, group_pair):
            rounded = jnp.dot(group_pair[0], group_pair[1], preferred_element_type=jnp.float32).astype(jnp.bfloat16)
            rounded = lax.optimization_barrier(rounded)
            return (running + rounded.astype(jnp.float32), None)
        running, unused = lax.scan(add_group, jnp.zeros((row_block.shape[0], D), jnp.float32), (hidden_groups, down_groups))
        return running.astype(jnp.bfloat16)
    expert_out = lax.map(one_expert, (slot_table, gate_proj, up_proj, down_proj))
    picked = expert_out[flat_expert, slot_index].astype(jnp.float32).reshape(TOKENS, 2, D)
    combined = lax.optimization_barrier(jnp.sum(expert_weights[:, :, None] * picked, axis=1))
    return (stream.astype(jnp.float32) + combined).astype(jnp.bfloat16)
```

```python
import functools

import jax
import jax.numpy as jnp
from jax import lax
from jax.experimental import pallas as pl
from jax.experimental.pallas import tpu as pltpu
from jax.sharding import PartitionSpec as P

epsilon = 1e-06


def rms_scaled(values_in):
    return values_in * lax.rsqrt(jnp.mean(values_in * values_in, axis=-1, keepdims=True) + epsilon)


def expert_partial(row_block, gate_matrix, up_matrix, down_matrix):
    gate_part = jnp.dot(row_block, gate_matrix, preferred_element_type=jnp.float32)
    up_part = jnp.dot(row_block, up_matrix, preferred_element_type=jnp.float32)
    hidden = (jax.nn.silu(gate_part) * up_part).astype(jnp.bfloat16)
    return jnp.dot(hidden, down_matrix, preferred_element_type=jnp.float32)


def choice_ranks(routes, experts_all):
    flat_routes = routes.reshape(routes.shape[:-2] + (-1,))
    onehot = (flat_routes[..., None] == jnp.arange(experts_all, dtype=jnp.int32)).astype(jnp.int32)
    before = jnp.cumsum(onehot, axis=-2) - onehot
    return jnp.sum(before * onehot, axis=-1).reshape(routes.shape)


def slot_tokens(slot_index, targets, missing):
    flat_slots = slot_index.reshape(-1)
    owners = jnp.arange(flat_slots.shape[0], dtype=jnp.int32) // 2
    matches = flat_slots[None, :] == jnp.arange(targets, dtype=jnp.int32)[:, None]
    owner_found = jnp.sum(jnp.where(matches, owners[None, :], 0), axis=1)
    return jnp.where(jnp.any(matches, axis=1), owner_found, missing)


def softplus_parts(scores):
    drops = -jnp.maximum(scores, 0.0) - jnp.log(1.0 + jnp.exp(-jnp.abs(scores)))
    return drops, scores + drops


def attend_block(query_ref, key_of, value_of, bias_of, mix_ref, carry_ref, head_size, diagonal):
    rows, width = query_ref.shape
    lanes = 128 if width % 128 == 0 else width
    per_group = lanes // head_size
    chunk = 128 if rows % 128 == 0 else rows
    later_row = lax.broadcasted_iota(jnp.int32, (rows, rows), 0)
    later_col = lax.broadcasted_iota(jnp.int32, (rows, rows), 1)
    suffix_of = jnp.where(later_row > later_col, 1.0, 0.0).astype(jnp.bfloat16)
    lane_head = lax.broadcasted_iota(jnp.int32, (1, lanes), 1) // head_size
    for group in range(width // lanes):
        cols = slice(group * lanes, (group + 1) * lanes)
        key_tile = key_of(cols)
        value_tile = value_of(cols)
        for inner in range(per_group):
            mine = lane_head == inner
            bias_row = bias_of(group * per_group + inner)
            for start in range(0, rows, chunk):
                span = slice(start, start + chunk)
                query = query_ref[span, cols] * jnp.asarray(head_size**-0.5, jnp.bfloat16)
                query = jnp.where(mine, query, jnp.zeros_like(query))
                scores = lax.dot_general(
                    query, key_tile, (((1,), (1,)), ((), ())), preferred_element_type=jnp.float32
                )
                scores = scores + bias_row
                drops, hits = softplus_parts(scores)
                if diagonal:
                    row_pos = start + lax.broadcasted_iota(jnp.int32, (chunk, rows), 0)
                    col_pos = lax.broadcasted_iota(jnp.int32, (chunk, rows), 1)
                    earlier = col_pos < row_pos
                    drops = jnp.where(earlier, drops, 0.0)
                high = drops.astype(jnp.bfloat16)
                low = (drops - high.astype(jnp.float32)).astype(jnp.bfloat16)
                suffix = jnp.dot(high, suffix_of, preferred_element_type=jnp.float32)
                suffix = suffix + jnp.dot(low, suffix_of, preferred_element_type=jnp.float32)
                within = jnp.exp(hits + suffix)
                if diagonal:
                    within = jnp.where(earlier, within, 0.0)
                part = jnp.dot(
                    within.astype(jnp.bfloat16), value_tile, preferred_element_type=jnp.float32
                )
                total = suffix[:, 0:1] + drops[:, 0:1]
                if diagonal:
                    mix_old = jnp.zeros((chunk, lanes), jnp.float32)
                    carry_old = mix_old
                    if inner > 0:
                        mix_old = mix_ref[span, cols]
                        carry_old = carry_ref[span, cols]
                    mix_ref[span, cols] = jnp.where(mine, part, mix_old)
                    carry_ref[span, cols] = jnp.where(mine, total, carry_old)
                else:
                    mix_old = mix_ref[span, cols]
                    carry_old = carry_ref[span, cols]
                    mix_ref[span, cols] = jnp.where(
                        mine, mix_old + jnp.exp(carry_old) * part, mix_old
                    )
                    carry_ref[span, cols] = jnp.where(mine, carry_old + total, carry_old)


def diagonal_kernel(head_size, query_ref, key_ref, value_ref, bias_ref, mix_ref, carry_ref):
    attend_block(
        query_ref,
        lambda cols: key_ref[:, cols],
        lambda cols: value_ref[:, cols],
        lambda head: bias_ref[head : head + 1, :],
        mix_ref,
        carry_ref,
        head_size,
        True,
    )


def earlier_kernel(
    head_size, query_ref, pack_ref, bias_ref, mix_in, carry_in, gain_ref, out_ref, mix_ref, carry_ref
):
    rows, width = query_ref.shape
    lanes = 128 if width % 128 == 0 else width
    mix_ref[...] = mix_in[...]
    carry_ref[...] = carry_in[...]
    own = lax.axis_index("sp")

    def visit(step, nothing):
        block = own - 1 - step
        attend_block(
            query_ref,
            lambda cols: pack_ref[block, :rows, cols],
            lambda cols: pack_ref[block, :rows, slice(width + cols.start, width + cols.stop)],
            lambda head: bias_ref[block, head : head + 1, :],
            mix_ref,
            carry_ref,
            head_size,
            False,
        )
        return nothing

    lax.fori_loop(0, own, visit, 0)
    lane_head = lax.broadcasted_iota(jnp.int32, (1, lanes), 1) // head_size
    for group in range(width // lanes):
        cols = slice(group * lanes, (group + 1) * lanes)
        mixture = mix_ref[:, cols]
        squares = mixture * mixture
        scaled = mixture
        for inner in range(lanes // head_size):
            mine = lane_head == inner
            mean = jnp.sum(jnp.where(mine, squares, 0.0), axis=1, keepdims=True) / head_size
            scaled = jnp.where(mine, mixture * lax.rsqrt(mean + epsilon), scaled)
        out_ref[:, cols] = (scaled * gain_ref[:, cols]).astype(jnp.bfloat16)


def attention(queries, keys, values, key_bias, head_gain):
    rows, width = queries.shape
    heads, head_size = head_gain.shape
    blocks = lax.axis_size("sp")
    bias_own = key_bias.T
    extra = -(-heads * rows // (2 * width))
    padded = -(-(rows + extra) // 8) * 8 - rows
    flat_bias = jnp.pad(bias_own.reshape(-1), (0, padded * 2 * width - heads * rows))
    packed = jnp.concatenate(
        [jnp.concatenate([keys, values], axis=1), flat_bias.reshape(padded, 2 * width)], axis=0
    )
    gathered = lax.all_gather(packed, "sp", axis=0)
    vmem = pl.BlockSpec(memory_space=pltpu.VMEM)
    state = jax.ShapeDtypeStruct((rows, width), jnp.float32)
    work = heads * rows * rows
    mix, carry = pl.pallas_call(
        functools.partial(diagonal_kernel, head_size),
        out_shape=[state, state],
        in_specs=[vmem] * 4,
        out_specs=[vmem] * 2,
        cost_estimate=pl.CostEstimate(flops=work * 2000, bytes_accessed=10**6, transcendentals=0),
    )(queries, keys, values, bias_own.astype(jnp.float32))
    bias_all = gathered[:, rows:].reshape(blocks, -1)[:, : heads * rows]
    bias_all = bias_all.reshape(blocks, heads, rows).astype(jnp.float32)
    return pl.pallas_call(
        functools.partial(earlier_kernel, head_size),
        out_shape=jax.ShapeDtypeStruct((rows, width), jnp.bfloat16),
        in_specs=[vmem] * 6,
        out_specs=vmem,
        scratch_shapes=[pltpu.VMEM((rows, width), jnp.float32)] * 2,
        cost_estimate=pl.CostEstimate(flops=work * 4000, bytes_accessed=10**6, transcendentals=0),
    )(queries, gathered, bias_all, mix, carry, head_gain.reshape(1, width))


class Places:
    def __init__(self):
        self.sp = lax.axis_index("sp")
        self.tp = lax.axis_index("tp")
        self.depth = lax.axis_size("tp") // 2
        self.z = self.tp // 2
        self.core = self.tp % 2
        self.col = self.sp % 2
        self.line = self.sp // 2
        self.across = self.line * 2 + 1 - self.col
        self.along = (1 - self.line) * 2 + self.col
        self.far = (1 - self.line) * 2 + 1 - self.col
        self.partner = (self.sp, self.z * 2 + 1 - self.core)
        self.x_next = (self.across, self.tp)
        self.y_next = (self.along, self.tp)

    def z_peer(self, step):
        return lax.rem(self.z + step, self.depth)

    def z_device(self, step):
        return (self.sp, self.z_peer(step) * 2 + self.core)

    def meet(self, wide):
        barrier = pltpu.get_barrier_semaphore()
        peers = [self.partner] + [self.z_device(step) for step in range(1, self.depth)]
        if wide:
            peers = peers + [self.x_next, self.y_next]
        for peer in peers:
            pl.semaphore_signal(
                barrier, inc=1, device_id=peer, device_id_type=pl.DeviceIdType.MESH
            )
        pl.semaphore_wait(barrier, len(peers))


def remote(source, target, send_sem, recv_sem, device):
    return pltpu.make_async_remote_copy(
        src_ref=source,
        dst_ref=target,
        send_sem=send_sem,
        recv_sem=recv_sem,
        device_id=device,
        device_id_type=pl.DeviceIdType.MESH,
    )


def add_into(target, first, *others):
    def one(z, nothing):
        total = first[z].astype(jnp.float32)
        for other in others:
            total = total + other[z].astype(jnp.float32)
        target[z] = total.astype(target.dtype)
        return nothing

    lax.fori_loop(0, target.shape[0], one, 0)


def finish_over_z(place, mine, z_recv, send_sems, recv_sems, base_ref, out_ref):
    copies = []
    order = [1] + list(range(place.depth - 1, 1, -1))
    for step in order:
        copy = remote(
            mine.at[place.z_peer(step)],
            z_recv.at[step - 1],
            send_sems.at[step - 1],
            recv_sems.at[step - 1],
            place.z_device(step),
        )
        copy.start()
        copies.append(copy)
    total = mine[place.z].astype(jnp.float32)
    for step, copy in zip(order, copies):
        copy.wait_recv()
        total = total + z_recv[step - 1].astype(jnp.float32)
    out_ref[...] = (base_ref[...].astype(jnp.float32) + total).astype(out_ref.dtype)
    for copy in copies:
        copy.wait_send()


def narrow_kernel(
    parts_ref, base_ref, out_ref, pair_recv, mine, z_recv, pair_send, pair_got, z_send, z_got
):
    place = Places()
    place.meet(False)
    copy = remote(
        parts_ref.at[1 - place.core], pair_recv, pair_send.at[0], pair_got.at[0], place.partner
    )
    copy.start()
    copy.wait_recv()
    add_into(mine, parts_ref.at[place.core], pair_recv)
    finish_over_z(place, mine, z_recv, z_send, z_got, base_ref, out_ref)
    copy.wait_send()


def scatter_sum(parts, base, out_dtype):
    rows, width = base.shape
    depth = lax.axis_size("tp") // 2
    vmem = pl.BlockSpec(memory_space=pltpu.VMEM)

    def room(*lead):
        return pltpu.VMEM(lead + (rows, width), jnp.bfloat16)

    def sems(count):
        return pltpu.SemaphoreType.DMA((count,))

    shaped = parts.reshape(depth, 2, rows, width).transpose(1, 0, 2, 3)
    return pl.pallas_call(
        narrow_kernel,
        out_shape=jax.ShapeDtypeStruct((rows, width), out_dtype),
        in_specs=[vmem] * 2,
        out_specs=vmem,
        scratch_shapes=[room(depth), room(depth), room(depth - 1)]
        + [sems(1), sems(1), sems(depth - 1), sems(depth - 1)],
        compiler_params=pltpu.CompilerParams(
            collective_id=0, has_side_effects=True, vmem_limit_bytes=60 * 2**20
        ),
    )(shaped, base)


class Sends:
    def __init__(self, sems):
        self.sems = sems
        self.made = []

    def start(self, source, target, recv_sem, device, when=None):
        copy = remote(source, target, self.sems.at[len(self.made)], recv_sem, device)
        self.made.append((copy, when))
        if when is None:
            copy.start()
        else:
            pl.when(when)(copy.start)

    def finish(self):
        for copy, when in self.made:
            if when is None:
                copy.wait_send()
            else:
                pl.when(when)(copy.wait_send)


def plane_order(z, depth, step):
    near = jnp.minimum(z, depth - 1 - z)
    if step % 2 == 1:
        swing = z - (step + 1) // 2
    else:
        swing = z + step // 2
    rest = jnp.where(z == near, step, depth - 1 - step)
    return jnp.where(step <= 2 * near, swing, rest)


def layer_kernel(
    own_ref,
    stream_ref,
    gate_ref,
    up_ref,
    down_ref,
    out_ref,
    rows_buf,
    pair_w,
    down_w,
    hidden,
    parts,
    pair_recv,
    x_far,
    y_far,
    x_near,
    y_near,
    x_last,
    y_last,
    totals,
    z_recv,
    local_sem,
    weight_sems,
    send_sems,
    z_got,
    x_got,
    y_got,
    far_got,
    side_got,
    pair_got,
    cross_got,
    z_sum_got,
):
    place = Places()
    depth, core, own_z = place.depth, place.core, place.z
    rows, width = out_ref.shape
    wide = own_ref.shape[1]
    count = 8 * rows
    half = width // 2
    cut = wide // 256 * 128
    hidden_width = hidden.shape[1]
    tile = 128
    copies = []
    for index in range(hidden_width // tile):
        for which, source in enumerate((gate_ref, up_ref)):
            copies.append(
                pltpu.make_async_copy(
                    source.at[:, pl.ds(index * tile, tile)],
                    pair_w.at[:, pl.ds((2 * index + which) * tile, tile)],
                    weight_sems.at[len(copies)],
                )
            )
    copies.append(pltpu.make_async_copy(down_ref, down_w, weight_sems.at[len(copies)]))
    for copy in copies:
        copy.start()
    place.meet(True)
    sends = Sends(send_sems)
    planes = [plane_order(own_z, depth, step) for step in range(depth)]
    front, back = pl.ds(0, cut), pl.ds(cut, wide - cut)
    left, right = pl.ds(0, half), pl.ds(half, half)
    z_up = (place.sp, (own_z + 1) * 2 + core)
    z_down = (place.sp, (own_z - 1) * 2 + core)
    has_up, has_down = own_z < depth - 1, own_z > 0

    def slot(step, seq):
        return rows_buf.at[planes[step], core, seq]

    def wait_for(target, sem):
        remote(target, target, send_sems.at[0], sem, place.partner).wait_recv()

    def to_partner(step, seq, source=None):
        target = slot(step, seq)
        sends.start(
            target if source is None else source,
            target,
            side_got.at[planes[step], seq],
            place.partner,
        )

    def own(step):
        plane = planes[step]
        target = slot(step, place.sp)
        source = own_ref
        if step > 0:
            wait_for(target, z_got.at[plane])
            source = target
            go_up = jnp.logical_and(has_up, plane < own_z)
            go_down = jnp.logical_and(has_down, plane > own_z)
        else:
            go_up, go_down = has_up, has_down
        if depth > 1:
            sends.start(source, target, z_got.at[plane], z_up, go_up)
            sends.start(source, target, z_got.at[plane], z_down, go_down)
        sends.start(source, target, x_got.at[plane], place.x_next)
        sends.start(source, target, y_got.at[plane], place.y_next)
        to_partner(step, place.sp, source)

    def relay(step):
        plane = planes[step]
        across, along = slot(step, place.across), slot(step, place.along)
        wait_for(across, x_got.at[plane])
        sends.start(across.at[:, front], across.at[:, front], far_got.at[plane, 0], place.y_next)
        wait_for(along, y_got.at[plane])
        sends.start(along.at[:, back], along.at[:, back], far_got.at[plane, 1], place.x_next)
        to_partner(step, place.across)
        to_partner(step, place.along)

    def far(step):
        plane = planes[step]
        target = slot(step, place.far)
        wait_for(target.at[:, front], far_got.at[plane, 0])
        wait_for(target.at[:, back], far_got.at[plane, 1])
        to_partner(step, place.far)

    def ready(step):
        plane = planes[step]
        for seq in (place.sp, place.across, place.along, place.far):
            wait_for(rows_buf.at[plane, 1 - core, seq], side_got.at[plane, seq])

    def compute(step):
        plane = planes[step]

        def open_tile(index, nothing):
            spot = pl.multiple_of(index * 2 * tile, 2 * tile)
            block = rows_buf[plane, :, :, :, :width].reshape(count, width)
            both = jnp.dot(
                block, pair_w[:, pl.ds(spot, 2 * tile)], preferred_element_type=jnp.float32
            )
            gate_part, up_part = both[:, :tile], both[:, tile:]
            value = gate_part / (1.0 + jnp.exp(-gate_part)) * up_part
            hidden[:, pl.ds(pl.multiple_of(index * tile, tile), tile)] = value.astype(jnp.bfloat16)
            return nothing

        lax.fori_loop(0, hidden_width // tile, open_tile, 0)
        lane = lax.broadcasted_iota(jnp.int32, (count, tile), 1)
        extra = rows_buf[plane, :, :, :, width:].reshape(count, tile).astype(jnp.float32)
        mine = jnp.logical_or(lane == place.sp, lane == place.sp + 4)
        weight = jnp.sum(jnp.where(mine, extra, 0.0), axis=1, keepdims=True)

        def down_tile(index, nothing):
            spot = pl.ds(pl.multiple_of(index * 2 * tile, 2 * tile), 2 * tile)
            share = jnp.dot(hidden[...], down_w[:, spot], preferred_element_type=jnp.float32)
            share = jnp.where(weight > 0.0, weight * share, 0.0).astype(jnp.bfloat16)
            parts[step, :, :, :, spot] = share.reshape(2, 4, rows, 2 * tile)
            return nothing

        lax.fori_loop(0, width // (2 * tile), down_tile, 0)
        sends.start(
            parts.at[step, 1 - core], pair_recv.at[step], pair_got.at[step], place.partner
        )

    def first_sum(step):
        wait_for(pair_recv.at[step], pair_got.at[step])
        add_into(parts.at[step, core], parts.at[step, core], pair_recv.at[step])
        mine = parts.at[step, core]
        got = cross_got.at[step]
        sends.start(mine.at[place.far, :, left], x_far.at[step], got.at[0], place.x_next)
        sends.start(mine.at[place.far, :, right], y_far.at[step], got.at[1], place.y_next)
        sends.start(mine.at[place.across, :, left], x_near.at[step], got.at[2], place.x_next)
        sends.start(mine.at[place.along, :, right], y_near.at[step], got.at[3], place.y_next)

    def plus(target, *others):
        total = target.astype(jnp.float32)
        for other in others:
            total = total + other.astype(jnp.float32)
        return total

    def second_sum(step):
        got = cross_got.at[step]
        wait_for(x_far.at[step], got.at[0])
        x_far[step] = plus(x_far[step], parts[step, core, place.along, :, left]).astype(jnp.bfloat16)
        sends.start(x_far.at[step], y_last.at[step], got.at[4], place.y_next)
        wait_for(y_far.at[step], got.at[1])
        y_far[step] = plus(y_far[step], parts[step, core, place.across, :, right]).astype(jnp.bfloat16)
        sends.start(y_far.at[step], x_last.at[step], got.at[5], place.x_next)

    def third_sum(step):
        got = cross_got.at[step]
        wait_for(x_near.at[step], got.at[2])
        wait_for(y_last.at[step], got.at[4])
        low = plus(parts[step, core, place.sp, :, left], x_near[step], y_last[step])
        wait_for(y_near.at[step], got.at[3])
        wait_for(x_last.at[step], got.at[5])
        high = plus(parts[step, core, place.sp, :, right], y_near[step], x_last[step])
        if step > 0:
            totals[step, :, left] = low.astype(jnp.bfloat16)
            totals[step, :, right] = high.astype(jnp.bfloat16)
            sends.start(
                totals.at[step],
                z_recv.at[own_z],
                z_sum_got.at[own_z],
                (place.sp, planes[step] * 2 + core),
            )
        else:
            for shift in range(1, depth):
                other = place.z_peer(shift)
                wait_for(z_recv.at[other], z_sum_got.at[other])
                low = plus(low, z_recv[other, :, left])
                high = plus(high, z_recv[other, :, right])
            out_ref[:, left] = plus(low, stream_ref[:, left]).astype(jnp.bfloat16)
            out_ref[:, right] = plus(high, stream_ref[:, right]).astype(jnp.bfloat16)

    local = pltpu.make_async_copy(own_ref, slot(0, place.sp), local_sem)
    local.start()
    own(0)
    own(1)
    relay(0)
    for step in range(2, depth):
        own(step)
        far(step - 2)
        relay(step - 1)
    for copy in copies:
        copy.wait()
    local.wait()
    order = list(range(1, depth)) + [0]
    for index, step in enumerate(order):
        if index == 1:
            relay(depth - 1)
        if step == depth - 2:
            far(depth - 2)
        if step == depth - 1:
            far(depth - 1)
        ready(step)
        compute(step)
        if index >= 1:
            second_sum(order[index - 1])
        if index >= 2:
            third_sum(order[index - 2])
        first_sum(step)
    second_sum(order[-1])
    third_sum(order[-2])
    third_sum(order[-1])
    sends.finish()


def expert_layer(own_rows, stream, gate_matrix, up_matrix, down_matrix):
    rows, width = stream.shape
    wide = own_rows.shape[1]
    depth = lax.axis_size("tp") // 2
    hidden_width = gate_matrix.shape[1]
    vmem = pl.BlockSpec(memory_space=pltpu.VMEM)
    anywhere = pl.BlockSpec(memory_space=pl.ANY)

    def room(*shape):
        return pltpu.VMEM(shape, jnp.bfloat16)

    def sems(*shape):
        return pltpu.SemaphoreType.DMA(shape)

    half = [room(depth, rows, width // 2)] * 6
    total_sends = depth * (5 + 4 + 1 + 1 + 4 + 2) + depth - 1
    return pl.pallas_call(
        layer_kernel,
        out_shape=jax.ShapeDtypeStruct((rows, width), jnp.bfloat16),
        in_specs=[vmem, vmem, anywhere, anywhere, anywhere],
        out_specs=vmem,
        scratch_shapes=[
            room(depth, 2, 4, rows, wide),
            room(width, 2 * hidden_width),
            room(hidden_width, width),
            room(8 * rows, hidden_width),
            room(depth, 2, 4, rows, width),
            room(depth, 4, rows, width),
        ]
        + half
        + [
            room(depth, rows, width),
            room(depth, rows, width),
            pltpu.SemaphoreType.DMA,
            sems(2 * (hidden_width // 128) + 1),
            sems(total_sends),
            sems(depth),
            sems(depth),
            sems(depth),
            sems(depth, 2),
            sems(depth, 4),
            sems(depth),
            sems(depth, 6),
            sems(depth),
        ],
        compiler_params=pltpu.CompilerParams(
            collective_id=1, has_side_effects=True, vmem_limit_bytes=60 * 2**20
        ),
    )(own_rows, stream, gate_matrix, up_matrix, down_matrix)


def on_device(
    queries,
    keys,
    values,
    key_bias,
    head_gain,
    out_weight,
    residual,
    norm_gain,
    gate_proj,
    up_proj,
    down_proj,
    expert_choice,
    expert_weights,
):
    rows_own = queries.shape[0]
    model_width = out_weight.shape[1]
    seq_devices = lax.axis_size("sp")
    head_devices = lax.axis_size("tp")
    row_share = rows_own // head_devices
    local_experts = gate_proj.shape[0]
    experts_all = local_experts * seq_devices
    capacity = 4 * rows_own // (head_devices * experts_all)
    dense = capacity >= row_share and seq_devices == 4 and head_devices % 4 == 0
    dense = dense and local_experts == 1 and head_devices >= 8
    if dense:
        named = expert_choice[:, :, None] == jnp.arange(experts_all, dtype=jnp.int32)
        own_weights = jnp.sum(jnp.where(named, expert_weights[:, :, None], 0.0), axis=1)
    attended = attention(queries, keys, values, key_bias, head_gain)
    shares = jnp.dot(attended, out_weight, preferred_element_type=jnp.float32)
    stream = scatter_sum(shares.astype(jnp.bfloat16), residual, jnp.bfloat16)
    normed = (rms_scaled(stream.astype(jnp.float32)) * norm_gain).astype(jnp.bfloat16)
    if dense:
        high = lax.reduce_precision(own_weights, 8, 7)
        blank = jnp.zeros((row_share, 128 - 2 * experts_all), jnp.bfloat16)
        extra = [high.astype(jnp.bfloat16), (own_weights - high).astype(jnp.bfloat16), blank]
        own_rows = jnp.concatenate([normed] + extra, axis=1)
        return expert_layer(own_rows, stream, gate_proj[0], up_proj[0], down_proj[0])
    own_slots = expert_choice * capacity + choice_ranks(expert_choice, experts_all)
    wanted = slot_tokens(own_slots, experts_all * capacity, row_share)
    outgoing = jnp.take(normed, wanted, axis=0, mode="fill", fill_value=0)
    arrived = lax.all_to_all(
        outgoing.reshape(seq_devices, local_experts, capacity, model_width),
        "sp",
        split_axis=0,
        concat_axis=0,
        tiled=True,
    )
    row_piece = lax.all_gather(arrived, "tp", axis=0, tiled=True)
    count_rows = row_piece.shape[0]
    partials = jnp.stack(
        [
            expert_partial(
                row_piece[:, 0].reshape(-1, model_width), gate_proj[0], up_proj[0], down_proj[0]
            ).reshape(count_rows, capacity, model_width)
        ],
        axis=1,
    )
    summed = lax.psum_scatter(partials.astype(jnp.bfloat16), "tp", scatter_dimension=0, tiled=True)
    returned = lax.all_to_all(summed, "sp", split_axis=0, concat_axis=0, tiled=True).reshape(
        experts_all * capacity, model_width
    )
    picked = jnp.take(returned, own_slots, axis=0).astype(jnp.float32)
    combined = jnp.sum(expert_weights[:, :, None] * picked, axis=1)
    return (stream.astype(jnp.float32) + combined).astype(jnp.bfloat16)


def solution(mesh):
    placed = (
        P("sp", "tp"),
        P("sp", "tp"),
        P("sp", "tp"),
        P("sp", "tp"),
        P("tp", None),
        P("tp", None),
        P(("sp", "tp"), None),
        P(),
        P("sp", None, "tp"),
        P("sp", None, "tp"),
        P("sp", "tp", None),
        P(("sp", "tp"), None),
        P(("sp", "tp"), None),
    )
    return jax.shard_map(
        on_device, mesh=mesh, in_specs=placed, out_specs=P(("sp", "tp"), None), check_vma=False
    )
```

```python
import functools
import types

import jax
import jax.numpy as jnp
from jax import lax
from jax.experimental import pallas as pl
from jax.experimental.pallas import tpu as pltpu
from jax.sharding import PartitionSpec as P

epsilon = 1e-06


def rms_scaled(values_in):
    return values_in * lax.rsqrt(jnp.mean(values_in * values_in, axis=-1, keepdims=True) + epsilon)


def expert_partial(row_block, gate_matrix, up_matrix, down_matrix):
    gate_part = jnp.dot(row_block, gate_matrix, preferred_element_type=jnp.float32)
    up_part = jnp.dot(row_block, up_matrix, preferred_element_type=jnp.float32)
    hidden = (jax.nn.silu(gate_part) * up_part).astype(jnp.bfloat16)
    return jnp.dot(hidden, down_matrix, preferred_element_type=jnp.float32)


def choice_ranks(routes, experts_all):
    flat_routes = routes.reshape(routes.shape[:-2] + (-1,))
    onehot = (flat_routes[..., None] == jnp.arange(experts_all, dtype=jnp.int32)).astype(jnp.int32)
    before = jnp.cumsum(onehot, axis=-2) - onehot
    return jnp.sum(before * onehot, axis=-1).reshape(routes.shape)


def slot_tokens(slot_index, targets, missing):
    flat_slots = slot_index.reshape(-1)
    owners = jnp.arange(flat_slots.shape[0], dtype=jnp.int32) // 2
    matches = flat_slots[None, :] == jnp.arange(targets, dtype=jnp.int32)[:, None]
    owner_found = jnp.sum(jnp.where(matches, owners[None, :], 0), axis=1)
    return jnp.where(jnp.any(matches, axis=1), owner_found, missing)


def softplus_parts(scores):
    drops = -jnp.maximum(scores, 0.0) - jnp.log(1.0 + jnp.exp(-jnp.abs(scores)))
    return drops, scores + drops


def block_weights(query, key_tile, bias_row, mine, later, diagonal):
    rows = query.shape[0]
    query = jnp.where(mine, query, jnp.zeros_like(query))
    scores = lax.dot_general(
        query, key_tile, (((1,), (1,)), ((), ())), preferred_element_type=jnp.float32
    )
    scores = scores + bias_row
    drops, hits = softplus_parts(scores)
    if diagonal:
        row_pos = lax.broadcasted_iota(jnp.int32, (rows, rows), 0)
        col_pos = lax.broadcasted_iota(jnp.int32, (rows, rows), 1)
        earlier = col_pos < row_pos
        drops = jnp.where(earlier, drops, 0.0)
    suffix = jnp.dot(drops.astype(jnp.bfloat16), later, preferred_element_type=jnp.float32)
    within = jnp.exp(hits + suffix)
    if diagonal:
        within = jnp.where(earlier, within, 0.0)
    return within.astype(jnp.bfloat16), suffix[:, 0:1] + drops[:, 0:1]


def attend(query_ref, key_of, value_of, bias_of, later_ref, part_ref, total_ref, head_size, diagonal, group):
    lanes = 128
    per_group = lanes // head_size
    lane_head = lax.broadcasted_iota(jnp.int32, (1, lanes), 1) // head_size
    cols = slice(group * lanes, (group + 1) * lanes)
    query = query_ref[:, cols] * jnp.asarray(head_size**-0.5, jnp.bfloat16)
    part_all, total_all = 0.0, 0.0
    for inner in range(per_group):
        mine = lane_head == inner
        weights, total = block_weights(
            query, key_of(cols), bias_of(group * per_group + inner), mine, later_ref[...], diagonal
        )
        part = jnp.dot(weights, value_of(cols), preferred_element_type=jnp.float32)
        part_all = jnp.where(mine, part, part_all)
        total_all = jnp.where(mine, total, total_all)
    part_ref[:, cols] = part_all
    total_ref[:, cols] = total_all


def attend_block(query_ref, key_of, value_of, bias_of, mix_ref, carry_ref, head_size, diagonal):
    rows, width = query_ref.shape
    lanes = 128 if width % 128 == 0 else width
    per_group = lanes // head_size
    chunk = 128 if rows % 128 == 0 else rows
    later_row = lax.broadcasted_iota(jnp.int32, (rows, rows), 0)
    later_col = lax.broadcasted_iota(jnp.int32, (rows, rows), 1)
    suffix_of = jnp.where(later_row > later_col, 1.0, 0.0).astype(jnp.bfloat16)
    lane_head = lax.broadcasted_iota(jnp.int32, (1, lanes), 1) // head_size
    for group in range(width // lanes):
        cols = slice(group * lanes, (group + 1) * lanes)
        key_tile = key_of(cols)
        value_tile = value_of(cols)
        for inner in range(per_group):
            mine = lane_head == inner
            bias_row = bias_of(group * per_group + inner)
            for start in range(0, rows, chunk):
                span = slice(start, start + chunk)
                query = query_ref[span, cols] * jnp.asarray(head_size**-0.5, jnp.bfloat16)
                query = jnp.where(mine, query, jnp.zeros_like(query))
                scores = lax.dot_general(
                    query, key_tile, (((1,), (1,)), ((), ())), preferred_element_type=jnp.float32
                )
                scores = scores + bias_row
                drops, hits = softplus_parts(scores)
                if diagonal:
                    row_pos = start + lax.broadcasted_iota(jnp.int32, (chunk, rows), 0)
                    col_pos = lax.broadcasted_iota(jnp.int32, (chunk, rows), 1)
                    earlier = col_pos < row_pos
                    drops = jnp.where(earlier, drops, 0.0)
                high = drops.astype(jnp.bfloat16)
                low = (drops - high.astype(jnp.float32)).astype(jnp.bfloat16)
                suffix = jnp.dot(high, suffix_of, preferred_element_type=jnp.float32)
                suffix = suffix + jnp.dot(low, suffix_of, preferred_element_type=jnp.float32)
                within = jnp.exp(hits + suffix)
                if diagonal:
                    within = jnp.where(earlier, within, 0.0)
                part = jnp.dot(
                    within.astype(jnp.bfloat16), value_tile, preferred_element_type=jnp.float32
                )
                total = suffix[:, 0:1] + drops[:, 0:1]
                if diagonal:
                    mix_old = jnp.zeros((chunk, lanes), jnp.float32)
                    carry_old = mix_old
                    if inner > 0:
                        mix_old = mix_ref[span, cols]
                        carry_old = carry_ref[span, cols]
                    mix_ref[span, cols] = jnp.where(mine, part, mix_old)
                    carry_ref[span, cols] = jnp.where(mine, total, carry_old)
                else:
                    mix_old = mix_ref[span, cols]
                    carry_old = carry_ref[span, cols]
                    mix_ref[span, cols] = jnp.where(
                        mine, mix_old + jnp.exp(carry_old) * part, mix_old
                    )
                    carry_ref[span, cols] = jnp.where(mine, carry_old + total, carry_old)


def diagonal_kernel(head_size, query_ref, key_ref, value_ref, bias_ref, mix_ref, carry_ref):
    attend_block(
        query_ref,
        lambda cols: key_ref[:, cols],
        lambda cols: value_ref[:, cols],
        lambda head: bias_ref[head : head + 1, :],
        mix_ref,
        carry_ref,
        head_size,
        True,
    )


def earlier_kernel(
    head_size, query_ref, pack_ref, bias_ref, mix_in, carry_in, gain_ref, out_ref, mix_ref, carry_ref
):
    rows, width = query_ref.shape
    lanes = 128 if width % 128 == 0 else width
    mix_ref[...] = mix_in[...]
    carry_ref[...] = carry_in[...]
    own = lax.axis_index("sp")

    def visit(step, nothing):
        block = own - 1 - step
        attend_block(
            query_ref,
            lambda cols: pack_ref[block, :rows, cols],
            lambda cols: pack_ref[block, :rows, slice(width + cols.start, width + cols.stop)],
            lambda head: bias_ref[block, head : head + 1, :],
            mix_ref,
            carry_ref,
            head_size,
            False,
        )
        return nothing

    lax.fori_loop(0, own, visit, 0)
    lane_head = lax.broadcasted_iota(jnp.int32, (1, lanes), 1) // head_size
    for group in range(width // lanes):
        cols = slice(group * lanes, (group + 1) * lanes)
        mixture = mix_ref[:, cols]
        squares = mixture * mixture
        scaled = mixture
        for inner in range(lanes // head_size):
            mine = lane_head == inner
            mean = jnp.sum(jnp.where(mine, squares, 0.0), axis=1, keepdims=True) / head_size
            scaled = jnp.where(mine, mixture * lax.rsqrt(mean + epsilon), scaled)
        out_ref[:, cols] = (scaled * gain_ref[:, cols]).astype(jnp.bfloat16)


def attention(queries, keys, values, key_bias, head_gain):
    rows, width = queries.shape
    heads, head_size = head_gain.shape
    blocks = lax.axis_size("sp")
    bias_own = key_bias.T
    extra = -(-heads * rows // (2 * width))
    padded = -(-(rows + extra) // 8) * 8 - rows
    flat_bias = jnp.pad(bias_own.reshape(-1), (0, padded * 2 * width - heads * rows))
    packed = jnp.concatenate(
        [jnp.concatenate([keys, values], axis=1), flat_bias.reshape(padded, 2 * width)], axis=0
    )
    gathered = lax.all_gather(packed, "sp", axis=0)
    vmem = pl.BlockSpec(memory_space=pltpu.VMEM)
    state = jax.ShapeDtypeStruct((rows, width), jnp.float32)
    work = heads * rows * rows
    mix, carry = pl.pallas_call(
        functools.partial(diagonal_kernel, head_size),
        out_shape=[state, state],
        in_specs=[vmem] * 4,
        out_specs=[vmem] * 2,
        cost_estimate=pl.CostEstimate(flops=work * 2000, bytes_accessed=10**6, transcendentals=0),
    )(queries, keys, values, bias_own.astype(jnp.float32))
    bias_all = gathered[:, rows:].reshape(blocks, -1)[:, : heads * rows]
    bias_all = bias_all.reshape(blocks, heads, rows).astype(jnp.float32)
    return pl.pallas_call(
        functools.partial(earlier_kernel, head_size),
        out_shape=jax.ShapeDtypeStruct((rows, width), jnp.bfloat16),
        in_specs=[vmem] * 6,
        out_specs=vmem,
        scratch_shapes=[pltpu.VMEM((rows, width), jnp.float32)] * 2,
        cost_estimate=pl.CostEstimate(flops=work * 4000, bytes_accessed=10**6, transcendentals=0),
    )(queries, gathered, bias_all, mix, carry, head_gain.reshape(1, width))


class Places:
    def __init__(self):
        self.sp = lax.axis_index("sp")
        self.tp = lax.axis_index("tp")
        self.depth = lax.axis_size("tp") // 2
        self.z = self.tp // 2
        self.core = self.tp % 2
        self.col = self.sp % 2
        self.line = self.sp // 2
        self.across = self.line * 2 + 1 - self.col
        self.along = (1 - self.line) * 2 + self.col
        self.far = (1 - self.line) * 2 + 1 - self.col
        self.partner = (self.sp, self.z * 2 + 1 - self.core)
        self.x_next = (self.across, self.tp)
        self.y_next = (self.along, self.tp)

    def z_peer(self, step):
        return lax.rem(self.z + step, self.depth)

    def z_device(self, step):
        return (self.sp, self.z_peer(step) * 2 + self.core)

    def meet(self, wide):
        barrier = pltpu.get_barrier_semaphore()
        peers = [self.partner] + [self.z_device(step) for step in range(1, self.depth)]
        if wide:
            peers = peers + [self.x_next, self.y_next]
        for peer in peers:
            pl.semaphore_signal(
                barrier, inc=1, device_id=peer, device_id_type=pl.DeviceIdType.MESH
            )
        pl.semaphore_wait(barrier, len(peers))


def remote(source, target, send_sem, recv_sem, device):
    return pltpu.make_async_remote_copy(
        src_ref=source,
        dst_ref=target,
        send_sem=send_sem,
        recv_sem=recv_sem,
        device_id=device,
        device_id_type=pl.DeviceIdType.MESH,
    )


def add_into(target, first, *others):
    def one(z, nothing):
        total = first[z].astype(jnp.float32)
        for other in others:
            total = total + other[z].astype(jnp.float32)
        target[z] = total.astype(target.dtype)
        return nothing

    lax.fori_loop(0, target.shape[0], one, 0)


def finish_over_z(place, mine, z_recv, send_sems, recv_sems, base_ref, out_ref):
    copies = []
    order = [1] + list(range(place.depth - 1, 1, -1))
    for step in order:
        copy = remote(
            mine.at[place.z_peer(step)],
            z_recv.at[step - 1],
            send_sems.at[step - 1],
            recv_sems.at[step - 1],
            place.z_device(step),
        )
        copy.start()
        copies.append(copy)
    total = mine[place.z].astype(jnp.float32)
    for step, copy in zip(order, copies):
        copy.wait_recv()
        total = total + z_recv[step - 1].astype(jnp.float32)
    out_ref[...] = (base_ref[...].astype(jnp.float32) + total).astype(out_ref.dtype)
    for copy in copies:
        copy.wait_send()


def narrow_kernel(
    parts_ref, base_ref, out_ref, pair_recv, mine, z_recv, pair_send, pair_got, z_send, z_got
):
    place = Places()
    place.meet(False)
    copy = remote(
        parts_ref.at[1 - place.core], pair_recv, pair_send.at[0], pair_got.at[0], place.partner
    )
    copy.start()
    copy.wait_recv()
    add_into(mine, parts_ref.at[place.core], pair_recv)
    finish_over_z(place, mine, z_recv, z_send, z_got, base_ref, out_ref)
    copy.wait_send()


def scatter_sum(parts, base, out_dtype):
    rows, width = base.shape
    depth = lax.axis_size("tp") // 2
    vmem = pl.BlockSpec(memory_space=pltpu.VMEM)

    def room(*lead):
        return pltpu.VMEM(lead + (rows, width), jnp.bfloat16)

    def sems(count):
        return pltpu.SemaphoreType.DMA((count,))

    shaped = parts.reshape(depth, 2, rows, width).transpose(1, 0, 2, 3)
    return pl.pallas_call(
        narrow_kernel,
        out_shape=jax.ShapeDtypeStruct((rows, width), out_dtype),
        in_specs=[vmem] * 2,
        out_specs=vmem,
        scratch_shapes=[room(depth), room(depth), room(depth - 1)]
        + [sems(1), sems(1), sems(depth - 1), sems(depth - 1)],
        compiler_params=pltpu.CompilerParams(
            collective_id=0, has_side_effects=True, vmem_limit_bytes=60 * 2**20
        ),
    )(shaped, base)


class Sends:
    def __init__(self, sems):
        self.sems = sems
        self.made = []

    def start(self, source, target, recv_sem, device, when=None):
        copy = remote(source, target, self.sems.at[len(self.made)], recv_sem, device)
        self.made.append((copy, when))
        if when is None:
            copy.start()
        else:
            pl.when(when)(copy.start)

    def finish(self):
        for copy, when in self.made:
            if when is None:
                copy.wait_send()
            else:
                pl.when(when)(copy.wait_send)


def plane_order(z, depth, step):
    near = jnp.minimum(z, depth - 1 - z)
    if step % 2 == 1:
        swing = z - (step + 1) // 2
    else:
        swing = z + step // 2
    rest = jnp.where(z == near, step, depth - 1 - step)
    return jnp.where(step <= 2 * near, swing, rest)


def layer_kernel(names, head_size, *refs):
    at = types.SimpleNamespace(**dict(zip(names, refs)), head_size=head_size)
    place = Places()
    depth, core, own_z = place.depth, place.core, place.z
    rows, width = at.out.shape
    count = 8 * rows
    half = width // 2
    hidden_width = at.hidden.shape[1]
    tile = 128
    sends = Sends(at.send_sems)
    planes = [plane_order(own_z, depth, step) for step in range(depth)]

    def wait_for(target, sem):
        remote(target, target, at.send_sems.at[0], sem, place.partner).wait_recv()

    attention_copies = []
    pieces = []
    for group in range(at.pack.shape[1]):
        cols = pl.ds(group * 128, 128)
        pieces.append((at.keys.at[:, cols], at.pack.at[place.sp, group, 0]))
        pieces.append((at.values.at[:, cols], at.pack.at[place.sp, group, 1]))
    for index, (source, target) in enumerate(
        pieces
        + [
            (at.queries, at.query_buf),
            (at.out_weight, at.out_w),
            (at.residual, at.base),
        ]
    ):
        copy = pltpu.make_async_copy(source, target, at.copy_sems.at[index])
        copy.start()
        attention_copies.append(copy)
    expert_copies = []
    for index in range(hidden_width // tile):
        for which, source in enumerate((at.gate, at.up)):
            expert_copies.append(
                pltpu.make_async_copy(
                    source.at[:, pl.ds(index * tile, tile)],
                    at.pair_w.at[:, pl.ds((2 * index + which) * tile, tile)],
                    at.weight_sems.at[len(expert_copies)],
                )
            )
    expert_copies.append(
        pltpu.make_async_copy(at.down, at.down_w, at.weight_sems.at[len(expert_copies)])
    )
    for copy in expert_copies:
        copy.start()
    place.meet(True)
    attention_stage(at, place, sends, wait_for, attention_copies)
    share_stage(at, place, sends, wait_for, planes)
    expert_stage(at, place, sends, wait_for, planes, expert_copies)
    sends.finish()


def down_rows(row, rows):
    lanes = row.shape[1]
    row_at = lax.broadcasted_iota(jnp.int32, (rows, lanes), 0)
    lane_at = lax.broadcasted_iota(jnp.int32, (rows, lanes), 1)
    return jnp.sum(jnp.where(row_at == lane_at, row, 0.0), axis=1, keepdims=True)


def attention_stage(at, place, sends, wait_for, copies):
    pack, biases, routes = at.pack, at.biases, at.routes
    groups, seq, lanes = pack.shape[1], pack.shape[3], pack.shape[4]
    size = at.head_size
    heads = groups * lanes // size
    own = place.sp

    def piece(block, group):
        return pack.at[block, group]

    for group in range(groups):
        copies[2 * group].wait()
        copies[2 * group + 1].wait()
        source = piece(own, group)
        sends.start(source, source, at.pack_x.at[own, group], place.x_next)
        sends.start(source, source, at.pack_y.at[own, group], place.y_next)
    biases[own, :heads, :] = at.key_bias[...].astype(jnp.float32)
    choice, amount = at.choice[...], at.amount[...]
    rows = choice.shape[1]
    routes[place.z, place.core, own] = jnp.zeros((8, lanes), jnp.float32)
    for expert in range(4):
        chosen = jnp.where(choice == expert, amount, 0.0)
        total = jnp.sum(chosen, axis=0, keepdims=True)
        routes[place.z, place.core, own, expert : expert + 1, :rows] = total
    mine = routes.at[place.z, place.core, own]
    for target, sem in ((biases.at[own], 0), (mine, 1)):
        sends.start(target, target, at.small_x.at[own, sem], place.x_next)
        sends.start(target, target, at.small_y.at[own, sem], place.y_next)
    row_at = lax.broadcasted_iota(jnp.int32, (seq, seq), 0)
    col_at = lax.broadcasted_iota(jnp.int32, (seq, seq), 1)
    later = at.later
    later[...] = jnp.where(row_at > col_at, 1.0, 0.0).astype(jnp.bfloat16)
    copies[2 * groups].wait()

    def visit(block, group, diagonal):
        attend(
            at.query_buf,
            lambda cols: pack[block, group, 0],
            lambda cols: pack[block, group, 1],
            lambda head: biases[block, head : head + 1, :],
            later,
            at.part.at[block],
            at.total.at[block],
            size,
            diagonal,
            group,
        )

    def earlier(block, group):
        @pl.when(block < own)
        def run():
            visit(block, group, False)

    across, along, far = place.across, place.along, place.far
    for group in range(groups):
        visit(own, group, True)
    for group in range(groups):
        from_x, from_y = piece(across, group), piece(along, group)
        wait_for(from_x, at.pack_x.at[across, group])
        if group < groups // 2:
            sends.start(from_x, from_x, at.pack_far.at[group], place.y_next)
        wait_for(from_y, at.pack_y.at[along, group])
        if group >= groups // 2:
            sends.start(from_y, from_y, at.pack_far.at[group], place.x_next)
        if group == 0:
            for target, sem in ((biases, 0), (routes.at[place.z, place.core], 1)):
                wait_for(target.at[across], at.small_x.at[across, sem])
                wait_for(target.at[along], at.small_y.at[along, sem])
                sends.start(
                    target.at[across], target.at[across], at.small_far.at[sem], place.y_next
                )
        earlier(across, group)
        earlier(along, group)
    for sem, target in enumerate((biases, routes.at[place.z, place.core])):
        wait_for(target.at[far], at.small_far.at[sem])
    mine = routes.at[place.z, place.core]
    sends.start(mine, mine, at.route_side.at[place.z], place.partner)
    for shift in range(1, place.depth):
        sends.start(mine, mine, at.route_z.at[place.z], place.z_device(shift))
    for group in range(groups):
        wait_for(piece(far, group), at.pack_far.at[group])
        earlier(far, group)
    for shift in range(1, place.depth):
        other = place.z_peer(shift)
        got = routes.at[other, place.core]
        wait_for(got, at.route_z.at[other])
        sends.start(got, got, at.route_side.at[other], place.partner)
    part, total = at.part, at.total

    def join(step, nothing):
        block = own - 1 - step
        part[own] = part[own] + jnp.exp(total[own]) * part[block]
        total[own] = total[own] + total[block]
        return nothing

    lax.fori_loop(0, own, join, 0)
    lane_head = lax.broadcasted_iota(jnp.int32, (1, lanes), 1) // size
    for group in range(groups):
        cols = slice(group * lanes, (group + 1) * lanes)
        mixture = part[own, :, cols]
        squares = mixture * mixture
        scaled = mixture
        for inner in range(lanes // size):
            chosen = lane_head == inner
            mean = jnp.sum(jnp.where(chosen, squares, 0.0), axis=1, keepdims=True) / size
            scaled = jnp.where(chosen, mixture * lax.rsqrt(mean + epsilon), scaled)
        first = group * (lanes // size)
        gains = [at.head_gain[first + inner : first + inner + 1, :] for inner in range(lanes // size)]
        gain = jnp.concatenate(gains, axis=1)
        at.attended[:, cols] = (scaled * gain).astype(jnp.bfloat16)
    copies[-2].wait()
    copies[-1].wait()


def share_stage(at, place, sends, wait_for, planes):
    rows, width = at.out.shape
    depth, core = place.depth, place.core
    shares, pair, z_recv = at.shares, at.share_pair, at.share_z
    tile = 512
    for start in range(0, width, tile):
        cols = slice(start, start + tile)
        share = jnp.dot(
            at.attended[...], at.out_w[:, cols], preferred_element_type=jnp.float32
        ).astype(jnp.bfloat16)
        for z in range(depth):
            for side in range(2):
                low = (2 * z + side) * rows
                shares[side, z, :, cols] = share[low : low + rows]
    order = planes[1:][::-1] + planes[:1]
    for plane in order:
        sends.start(
            shares.at[1 - core, plane], pair.at[plane], at.share_side.at[plane], place.partner
        )
    for index, plane in enumerate(order):
        wait_for(pair.at[plane], at.share_side.at[plane])
        total = shares[core, plane].astype(jnp.float32) + pair[plane].astype(jnp.float32)
        if index < depth - 1:
            shares[core, plane] = total.astype(jnp.bfloat16)
            sends.start(
                shares.at[core, plane],
                z_recv.at[place.z],
                at.share_got.at[place.z],
                (place.sp, plane * 2 + core),
            )
    total = total + at.base[...].astype(jnp.float32)
    for plane in planes[1:]:
        wait_for(z_recv.at[plane], at.share_got.at[plane])
        total = total + z_recv[plane].astype(jnp.float32)
    stream = total.astype(jnp.bfloat16)
    at.stream[...] = stream
    normed = rms_scaled(stream.astype(jnp.float32)) * at.norm_gain[...]
    at.normed[...] = normed.astype(jnp.bfloat16)
    for plane in planes:
        side = at.routes.at[plane, 1 - core]
        wait_for(side, at.route_side.at[plane])


def expert_stage(at, place, sends, wait_for, planes, copies):
    depth, core, own_z = place.depth, place.core, place.z
    out_ref, own_ref, stream_ref = at.out, at.normed, at.stream
    rows_buf, pair_w, down_w, hidden = at.rows_buf, at.pair_w, at.down_w, at.hidden
    parts, pair_recv, totals, z_recv = at.parts, at.pair_recv, at.totals, at.z_recv
    x_far, y_far, x_near, y_near = at.x_far, at.y_far, at.x_near, at.y_near
    x_last, y_last, routes = at.x_last, at.y_last, at.routes
    local_sem, z_got, x_got, y_got = at.local_sem, at.z_got, at.x_got, at.y_got
    far_got, side_got, pair_got = at.far_got, at.side_got, at.pair_got
    cross_got, z_sum_got = at.cross_got, at.z_sum_got
    rows, width = out_ref.shape
    count = 8 * rows
    half = width // 2
    hidden_width = hidden.shape[1]
    tile = 128
    front, back = pl.ds(0, half), pl.ds(half, half)
    left, right = pl.ds(0, half), pl.ds(half, half)
    z_up = (place.sp, (own_z + 1) * 2 + core)
    z_down = (place.sp, (own_z - 1) * 2 + core)
    has_up, has_down = own_z < depth - 1, own_z > 0

    def slot(step, seq):
        return rows_buf.at[planes[step], core, seq]

    def to_partner(step, seq, source=None):
        target = slot(step, seq)
        sends.start(
            target if source is None else source,
            target,
            side_got.at[planes[step], seq],
            place.partner,
        )

    def own(step):
        plane = planes[step]
        target = slot(step, place.sp)
        source = own_ref
        if step > 0:
            wait_for(target, z_got.at[plane])
            source = target
            go_up = jnp.logical_and(has_up, plane < own_z)
            go_down = jnp.logical_and(has_down, plane > own_z)
        else:
            go_up, go_down = has_up, has_down
        if depth > 1:
            sends.start(source, target, z_got.at[plane], z_up, go_up)
            sends.start(source, target, z_got.at[plane], z_down, go_down)
        sends.start(source, target, x_got.at[plane], place.x_next)
        sends.start(source, target, y_got.at[plane], place.y_next)
        to_partner(step, place.sp, source)

    def relay(step):
        plane = planes[step]
        across, along = slot(step, place.across), slot(step, place.along)
        wait_for(across, x_got.at[plane])
        sends.start(across.at[:, front], across.at[:, front], far_got.at[plane, 0], place.y_next)
        wait_for(along, y_got.at[plane])
        sends.start(along.at[:, back], along.at[:, back], far_got.at[plane, 1], place.x_next)
        to_partner(step, place.across)
        to_partner(step, place.along)

    def far(step):
        plane = planes[step]
        target = slot(step, place.far)
        wait_for(target.at[:, front], far_got.at[plane, 0])
        wait_for(target.at[:, back], far_got.at[plane, 1])
        to_partner(step, place.far)

    def ready(step):
        plane = planes[step]
        for seq in (place.sp, place.across, place.along, place.far):
            wait_for(rows_buf.at[plane, 1 - core, seq], side_got.at[plane, seq])

    def open_tiles(step, low, high):
        plane = planes[step]
        pieces = []
        for side in range(2):
            for seq in range(4):
                row = routes[plane, side, seq, pl.ds(place.sp, 1), :]
                pieces.append(down_rows(row, rows))
        weight = jnp.concatenate(pieces, axis=0)
        block = rows_buf[plane].reshape(count, width)
        for index in range(low, high):
            both = jnp.dot(
                block,
                pair_w[:, 2 * index * tile : 2 * (index + 1) * tile],
                preferred_element_type=jnp.float32,
            )
            gate_part, up_part = both[:, :tile], both[:, tile:]
            value = gate_part / (1.0 + jnp.exp(-gate_part)) * up_part
            value = jnp.where(weight > 0.0, weight * value, 0.0)
            hidden[:, index * tile : (index + 1) * tile] = value.astype(jnp.bfloat16)

    def down_half(step, side):
        spot = right if side else left
        share = jnp.dot(hidden[...], down_w[:, spot], preferred_element_type=jnp.float32)
        parts[step, :, :, :, spot] = share.astype(jnp.bfloat16).reshape(2, 4, rows, half)
        sends.start(
            parts.at[step, 1 - core, :, :, spot],
            pair_recv.at[step, :, :, spot],
            pair_got.at[step, side],
            place.partner,
        )

    def pair_sum(step):
        for side, spot in enumerate((left, right)):
            wait_for(pair_recv.at[step, :, :, spot], pair_got.at[step, side])
        add_into(parts.at[step, core], parts.at[step, core], pair_recv.at[step])

    def first_sends(step):
        mine = parts.at[step, core]
        got = cross_got.at[step]
        sends.start(mine.at[place.far, :, left], x_far.at[step], got.at[0], place.x_next)
        sends.start(mine.at[place.far, :, right], y_far.at[step], got.at[1], place.y_next)
        sends.start(mine.at[place.across, :, left], x_near.at[step], got.at[2], place.x_next)
        sends.start(mine.at[place.along, :, right], y_near.at[step], got.at[3], place.y_next)

    def plus(target, *others):
        total = target.astype(jnp.float32)
        for other in others:
            total = total + other.astype(jnp.float32)
        return total

    def second_sum(step):
        got = cross_got.at[step]
        wait_for(x_far.at[step], got.at[0])
        x_far[step] = plus(x_far[step], parts[step, core, place.along, :, left]).astype(jnp.bfloat16)
        sends.start(x_far.at[step], y_last.at[step], got.at[4], place.y_next)
        wait_for(y_far.at[step], got.at[1])
        y_far[step] = plus(y_far[step], parts[step, core, place.across, :, right]).astype(jnp.bfloat16)
        sends.start(y_far.at[step], x_last.at[step], got.at[5], place.x_next)

    def third_sum(step):
        got = cross_got.at[step]
        wait_for(x_near.at[step], got.at[2])
        wait_for(y_last.at[step], got.at[4])
        low = plus(parts[step, core, place.sp, :, left], x_near[step], y_last[step])
        wait_for(y_near.at[step], got.at[3])
        wait_for(x_last.at[step], got.at[5])
        high = plus(parts[step, core, place.sp, :, right], y_near[step], x_last[step])
        if step > 0:
            totals[step, :, left] = low.astype(jnp.bfloat16)
            totals[step, :, right] = high.astype(jnp.bfloat16)
            sends.start(
                totals.at[step],
                z_recv.at[own_z],
                z_sum_got.at[own_z],
                (place.sp, planes[step] * 2 + core),
            )
        else:
            for shift in range(1, depth):
                other = place.z_peer(shift)
                wait_for(z_recv.at[other], z_sum_got.at[other])
                low = plus(low, z_recv[other, :, left])
                high = plus(high, z_recv[other, :, right])
            out_ref[:, left] = plus(low, stream_ref[:, left]).astype(jnp.bfloat16)
            out_ref[:, right] = plus(high, stream_ref[:, right]).astype(jnp.bfloat16)

    local = pltpu.make_async_copy(own_ref, slot(0, place.sp), local_sem)
    local.start()
    tiles = hidden_width // tile
    some = (tiles + 1) // 2
    own(0)
    own(1)
    relay(0)
    own(2)
    far(0)
    relay(1)
    for copy in copies:
        copy.wait()
    local.wait()
    last = depth - 1
    for step in range(depth):
        if step > 0:
            far(step)
        ready(step)
        open_tiles(step, 0, some)
        if step + 3 <= last:
            own(step + 3)
        if step == 1:
            pair_sum(0)
        if step >= 2:
            pair_sum(step - 1)
            first_sends(step - 1)
        open_tiles(step, some, tiles)
        if step >= 3:
            third_sum(step - 2)
        down_half(step, 0)
        if step + 2 <= last:
            relay(step + 2)
        down_half(step, 1)
        if step >= 2:
            second_sum(step - 1)
    pair_sum(last)
    first_sends(last)
    first_sends(0)
    third_sum(last - 1)
    second_sum(last)
    second_sum(0)
    third_sum(last)
    third_sum(0)


def layer(arrays, held, head_size):
    at = types.SimpleNamespace(**arrays)
    rows, width = at.residual.shape
    seq, part_width = at.queries.shape
    hidden_width = at.gate.shape[1]
    depth = lax.axis_size("tp") // 2
    groups = part_width // 128
    vmem = pl.BlockSpec(memory_space=pltpu.VMEM)
    anywhere = pl.BlockSpec(memory_space=pl.ANY)

    def room(*shape):
        return pltpu.VMEM(shape, jnp.bfloat16)

    def wide_room(*shape):
        return pltpu.VMEM(shape, jnp.float32)

    def sems(*shape):
        return pltpu.SemaphoreType.DMA(shape)

    half = room(depth, rows, width // 2)
    total_sends = depth * (5 + 4 + 1 + 2 + 4 + 2) + depth - 1
    total_sends = total_sends + 3 * groups + 6 + 1 + 2 * (depth - 1) + 2 * depth - 1
    scratch = dict(
        pack=room(4, groups, 2, seq, 128),
        query_buf=room(seq, part_width),
        out_w=room(part_width, width),
        base=room(rows, width),
        biases=wide_room(4, 8, seq),
        routes=wide_room(depth, 2, 4, 8, 128),
        later=room(seq, seq),
        part=wide_room(4, seq, part_width),
        total=wide_room(4, seq, part_width),
        attended=room(seq, part_width),
        shares=room(2, depth, rows, width),
        share_pair=room(depth, rows, width),
        share_z=room(depth, rows, width),
        stream=room(rows, width),
        normed=room(rows, width),
        rows_buf=room(depth, 2, 4, rows, width),
        pair_w=room(width, 2 * hidden_width),
        down_w=room(hidden_width, width),
        hidden=room(8 * rows, hidden_width),
        parts=room(depth, 2, 4, rows, width),
        pair_recv=room(depth, 4, rows, width),
        x_far=half,
        y_far=half,
        x_near=half,
        y_near=half,
        x_last=half,
        y_last=half,
        totals=room(depth, rows, width),
        z_recv=room(depth, rows, width),
        send_sems=sems(total_sends),
        copy_sems=sems(2 * groups + 3),
        weight_sems=sems(2 * (hidden_width // 128) + 1),
        pack_x=sems(4, groups),
        pack_y=sems(4, groups),
        pack_far=sems(groups),
        small_x=sems(4, 2),
        small_y=sems(4, 2),
        small_far=sems(2),
        route_side=sems(depth),
        route_z=sems(depth),
        share_side=sems(depth),
        share_got=sems(depth),
        local_sem=pltpu.SemaphoreType.DMA,
        z_got=sems(depth),
        x_got=sems(depth),
        y_got=sems(depth),
        far_got=sems(depth, 2),
        side_got=sems(depth, 4),
        pair_got=sems(depth, 2),
        cross_got=sems(depth, 6),
        z_sum_got=sems(depth),
    )
    names = list(arrays) + ["out"] + list(scratch)

    def body(*refs):
        layer_kernel(names, head_size, *refs)

    return pl.pallas_call(
        body,
        out_shape=jax.ShapeDtypeStruct((rows, width), jnp.bfloat16),
        in_specs=[anywhere] * held + [vmem] * (len(arrays) - held),
        out_specs=vmem,
        scratch_shapes=list(scratch.values()),
        compiler_params=pltpu.CompilerParams(
            collective_id=1, has_side_effects=True, vmem_limit_bytes=60 * 2**20
        ),
    )(*arrays.values())


def on_device(
    queries,
    keys,
    values,
    key_bias,
    head_gain,
    out_weight,
    residual,
    norm_gain,
    gate_proj,
    up_proj,
    down_proj,
    expert_choice,
    expert_weights,
):
    rows_own = queries.shape[0]
    model_width = out_weight.shape[1]
    seq_devices = lax.axis_size("sp")
    head_devices = lax.axis_size("tp")
    row_share = rows_own // head_devices
    local_experts = gate_proj.shape[0]
    experts_all = local_experts * seq_devices
    capacity = 4 * rows_own // (head_devices * experts_all)
    dense = capacity >= row_share and seq_devices == 4 and head_devices % 4 == 0
    dense = dense and local_experts == 1 and head_devices >= 8 and experts_all == 4
    dense = dense and rows_own % 128 == 0 and row_share <= 128 and queries.shape[1] % 256 == 0
    if dense:
        arrays = dict(
            keys=keys,
            values=values,
            queries=queries,
            out_weight=out_weight,
            residual=residual,
            gate=gate_proj[0],
            up=up_proj[0],
            down=down_proj[0],
            key_bias=key_bias.T,
            head_gain=head_gain,
            norm_gain=norm_gain.reshape(1, -1),
            choice=expert_choice.T,
            amount=expert_weights.T,
        )
        return layer(arrays, 8, head_gain.shape[1])
    attended = attention(queries, keys, values, key_bias, head_gain)
    shares = jnp.dot(attended, out_weight, preferred_element_type=jnp.float32)
    stream = scatter_sum(shares.astype(jnp.bfloat16), residual, jnp.bfloat16)
    normed = (rms_scaled(stream.astype(jnp.float32)) * norm_gain).astype(jnp.bfloat16)
    own_slots = expert_choice * capacity + choice_ranks(expert_choice, experts_all)
    wanted = slot_tokens(own_slots, experts_all * capacity, row_share)
    outgoing = jnp.take(normed, wanted, axis=0, mode="fill", fill_value=0)
    arrived = lax.all_to_all(
        outgoing.reshape(seq_devices, local_experts, capacity, model_width),
        "sp",
        split_axis=0,
        concat_axis=0,
        tiled=True,
    )
    row_piece = lax.all_gather(arrived, "tp", axis=0, tiled=True)
    count_rows = row_piece.shape[0]
    partials = jnp.stack(
        [
            expert_partial(
                row_piece[:, 0].reshape(-1, model_width), gate_proj[0], up_proj[0], down_proj[0]
            ).reshape(count_rows, capacity, model_width)
        ],
        axis=1,
    )
    summed = lax.psum_scatter(partials.astype(jnp.bfloat16), "tp", scatter_dimension=0, tiled=True)
    returned = lax.all_to_all(summed, "sp", split_axis=0, concat_axis=0, tiled=True).reshape(
        experts_all * capacity, model_width
    )
    picked = jnp.take(returned, own_slots, axis=0).astype(jnp.float32)
    combined = jnp.sum(expert_weights[:, :, None] * picked, axis=1)
    return (stream.astype(jnp.float32) + combined).astype(jnp.bfloat16)


def solution(mesh):
    placed = (
        P("sp", "tp"),
        P("sp", "tp"),
        P("sp", "tp"),
        P("sp", "tp"),
        P("tp", None),
        P("tp", None),
        P(("sp", "tp"), None),
        P(),
        P("sp", None, "tp"),
        P("sp", None, "tp"),
        P("sp", "tp", None),
        P(("sp", "tp"), None),
        P(("sp", "tp"), None),
    )
    return jax.shard_map(
        on_device, mesh=mesh, in_specs=placed, out_specs=P(("sp", "tp"), None), check_vma=False
    )
```

```python
import functools
import types

import jax
import jax.numpy as jnp
from jax import lax
from jax.experimental import pallas as pl
from jax.experimental.pallas import tpu as pltpu
from jax.sharding import PartitionSpec as P

epsilon = 1e-06


def rms_scaled(values_in):
    return values_in * lax.rsqrt(jnp.mean(values_in * values_in, axis=-1, keepdims=True) + epsilon)


def expert_partial(row_block, gate_matrix, up_matrix, down_matrix):
    gate_part = jnp.dot(row_block, gate_matrix, preferred_element_type=jnp.float32)
    up_part = jnp.dot(row_block, up_matrix, preferred_element_type=jnp.float32)
    hidden = (jax.nn.silu(gate_part) * up_part).astype(jnp.bfloat16)
    return jnp.dot(hidden, down_matrix, preferred_element_type=jnp.float32)


def choice_ranks(routes, experts_all):
    flat_routes = routes.reshape(routes.shape[:-2] + (-1,))
    onehot = (flat_routes[..., None] == jnp.arange(experts_all, dtype=jnp.int32)).astype(jnp.int32)
    before = jnp.cumsum(onehot, axis=-2) - onehot
    return jnp.sum(before * onehot, axis=-1).reshape(routes.shape)


def slot_tokens(slot_index, targets, missing):
    flat_slots = slot_index.reshape(-1)
    owners = jnp.arange(flat_slots.shape[0], dtype=jnp.int32) // 2
    matches = flat_slots[None, :] == jnp.arange(targets, dtype=jnp.int32)[:, None]
    owner_found = jnp.sum(jnp.where(matches, owners[None, :], 0), axis=1)
    return jnp.where(jnp.any(matches, axis=1), owner_found, missing)


def softplus_parts(scores):
    drops = -jnp.maximum(scores, 0.0) - jnp.log(1.0 + jnp.exp(-jnp.abs(scores)))
    return drops, scores + drops


def block_weights(query, key_tile, bias_row, mine, later, diagonal):
    rows = query.shape[0]
    query = jnp.where(mine, query, jnp.zeros_like(query))
    scores = lax.dot_general(
        query, key_tile, (((1,), (1,)), ((), ())), preferred_element_type=jnp.float32
    )
    scores = scores + bias_row
    drops, hits = softplus_parts(scores)
    if diagonal:
        row_pos = lax.broadcasted_iota(jnp.int32, (rows, rows), 0)
        col_pos = lax.broadcasted_iota(jnp.int32, (rows, rows), 1)
        earlier = col_pos < row_pos
        drops = jnp.where(earlier, drops, 0.0)
    suffix = jnp.dot(drops.astype(jnp.bfloat16), later, preferred_element_type=jnp.float32)
    within = jnp.exp(hits + suffix)
    if diagonal:
        within = jnp.where(earlier, within, 0.0)
    return within.astype(jnp.bfloat16), suffix[:, 0:1] + drops[:, 0:1]


def attend(query_ref, key_of, value_of, bias_of, later_ref, part_ref, total_ref, head_size, diagonal, group):
    lanes = 128
    per_group = lanes // head_size
    lane_head = lax.broadcasted_iota(jnp.int32, (1, lanes), 1) // head_size
    cols = slice(group * lanes, (group + 1) * lanes)
    query = query_ref[:, cols] * jnp.asarray(head_size**-0.5, jnp.bfloat16)
    part_all, total_all = 0.0, 0.0
    for inner in range(per_group):
        mine = lane_head == inner
        weights, total = block_weights(
            query, key_of(cols), bias_of(group * per_group + inner), mine, later_ref[...], diagonal
        )
        part = jnp.dot(weights, value_of(cols), preferred_element_type=jnp.float32)
        part_all = jnp.where(mine, part, part_all)
        total_all = jnp.where(mine, total, total_all)
    part_ref[:, cols] = part_all
    total_ref[:, cols] = total_all


def attend_block(query_ref, key_of, value_of, bias_of, mix_ref, carry_ref, head_size, diagonal):
    rows, width = query_ref.shape
    lanes = 128 if width % 128 == 0 else width
    per_group = lanes // head_size
    chunk = 128 if rows % 128 == 0 else rows
    later_row = lax.broadcasted_iota(jnp.int32, (rows, rows), 0)
    later_col = lax.broadcasted_iota(jnp.int32, (rows, rows), 1)
    suffix_of = jnp.where(later_row > later_col, 1.0, 0.0).astype(jnp.bfloat16)
    lane_head = lax.broadcasted_iota(jnp.int32, (1, lanes), 1) // head_size
    for group in range(width // lanes):
        cols = slice(group * lanes, (group + 1) * lanes)
        key_tile = key_of(cols)
        value_tile = value_of(cols)
        for inner in range(per_group):
            mine = lane_head == inner
            bias_row = bias_of(group * per_group + inner)
            for start in range(0, rows, chunk):
                span = slice(start, start + chunk)
                query = query_ref[span, cols] * jnp.asarray(head_size**-0.5, jnp.bfloat16)
                query = jnp.where(mine, query, jnp.zeros_like(query))
                scores = lax.dot_general(
                    query, key_tile, (((1,), (1,)), ((), ())), preferred_element_type=jnp.float32
                )
                scores = scores + bias_row
                drops, hits = softplus_parts(scores)
                if diagonal:
                    row_pos = start + lax.broadcasted_iota(jnp.int32, (chunk, rows), 0)
                    col_pos = lax.broadcasted_iota(jnp.int32, (chunk, rows), 1)
                    earlier = col_pos < row_pos
                    drops = jnp.where(earlier, drops, 0.0)
                high = drops.astype(jnp.bfloat16)
                low = (drops - high.astype(jnp.float32)).astype(jnp.bfloat16)
                suffix = jnp.dot(high, suffix_of, preferred_element_type=jnp.float32)
                suffix = suffix + jnp.dot(low, suffix_of, preferred_element_type=jnp.float32)
                within = jnp.exp(hits + suffix)
                if diagonal:
                    within = jnp.where(earlier, within, 0.0)
                part = jnp.dot(
                    within.astype(jnp.bfloat16), value_tile, preferred_element_type=jnp.float32
                )
                total = suffix[:, 0:1] + drops[:, 0:1]
                if diagonal:
                    mix_old = jnp.zeros((chunk, lanes), jnp.float32)
                    carry_old = mix_old
                    if inner > 0:
                        mix_old = mix_ref[span, cols]
                        carry_old = carry_ref[span, cols]
                    mix_ref[span, cols] = jnp.where(mine, part, mix_old)
                    carry_ref[span, cols] = jnp.where(mine, total, carry_old)
                else:
                    mix_old = mix_ref[span, cols]
                    carry_old = carry_ref[span, cols]
                    mix_ref[span, cols] = jnp.where(
                        mine, mix_old + jnp.exp(carry_old) * part, mix_old
                    )
                    carry_ref[span, cols] = jnp.where(mine, carry_old + total, carry_old)


def diagonal_kernel(head_size, query_ref, key_ref, value_ref, bias_ref, mix_ref, carry_ref):
    attend_block(
        query_ref,
        lambda cols: key_ref[:, cols],
        lambda cols: value_ref[:, cols],
        lambda head: bias_ref[head : head + 1, :],
        mix_ref,
        carry_ref,
        head_size,
        True,
    )


def earlier_kernel(
    head_size, query_ref, pack_ref, bias_ref, mix_in, carry_in, gain_ref, out_ref, mix_ref, carry_ref
):
    rows, width = query_ref.shape
    lanes = 128 if width % 128 == 0 else width
    mix_ref[...] = mix_in[...]
    carry_ref[...] = carry_in[...]
    own = lax.axis_index("sp")

    def visit(step, nothing):
        block = own - 1 - step
        attend_block(
            query_ref,
            lambda cols: pack_ref[block, :rows, cols],
            lambda cols: pack_ref[block, :rows, slice(width + cols.start, width + cols.stop)],
            lambda head: bias_ref[block, head : head + 1, :],
            mix_ref,
            carry_ref,
            head_size,
            False,
        )
        return nothing

    lax.fori_loop(0, own, visit, 0)
    lane_head = lax.broadcasted_iota(jnp.int32, (1, lanes), 1) // head_size
    for group in range(width // lanes):
        cols = slice(group * lanes, (group + 1) * lanes)
        mixture = mix_ref[:, cols]
        squares = mixture * mixture
        scaled = mixture
        for inner in range(lanes // head_size):
            mine = lane_head == inner
            mean = jnp.sum(jnp.where(mine, squares, 0.0), axis=1, keepdims=True) / head_size
            scaled = jnp.where(mine, mixture * lax.rsqrt(mean + epsilon), scaled)
        out_ref[:, cols] = (scaled * gain_ref[:, cols]).astype(jnp.bfloat16)


def attention(queries, keys, values, key_bias, head_gain):
    rows, width = queries.shape
    heads, head_size = head_gain.shape
    blocks = lax.axis_size("sp")
    bias_own = key_bias.T
    extra = -(-heads * rows // (2 * width))
    padded = -(-(rows + extra) // 8) * 8 - rows
    flat_bias = jnp.pad(bias_own.reshape(-1), (0, padded * 2 * width - heads * rows))
    packed = jnp.concatenate(
        [jnp.concatenate([keys, values], axis=1), flat_bias.reshape(padded, 2 * width)], axis=0
    )
    gathered = lax.all_gather(packed, "sp", axis=0)
    vmem = pl.BlockSpec(memory_space=pltpu.VMEM)
    state = jax.ShapeDtypeStruct((rows, width), jnp.float32)
    work = heads * rows * rows
    mix, carry = pl.pallas_call(
        functools.partial(diagonal_kernel, head_size),
        out_shape=[state, state],
        in_specs=[vmem] * 4,
        out_specs=[vmem] * 2,
        cost_estimate=pl.CostEstimate(flops=work * 2000, bytes_accessed=10**6, transcendentals=0),
    )(queries, keys, values, bias_own.astype(jnp.float32))
    bias_all = gathered[:, rows:].reshape(blocks, -1)[:, : heads * rows]
    bias_all = bias_all.reshape(blocks, heads, rows).astype(jnp.float32)
    return pl.pallas_call(
        functools.partial(earlier_kernel, head_size),
        out_shape=jax.ShapeDtypeStruct((rows, width), jnp.bfloat16),
        in_specs=[vmem] * 6,
        out_specs=vmem,
        scratch_shapes=[pltpu.VMEM((rows, width), jnp.float32)] * 2,
        cost_estimate=pl.CostEstimate(flops=work * 4000, bytes_accessed=10**6, transcendentals=0),
    )(queries, gathered, bias_all, mix, carry, head_gain.reshape(1, width))


class Places:
    def __init__(self):
        self.sp = lax.axis_index("sp")
        self.tp = lax.axis_index("tp")
        self.depth = lax.axis_size("tp") // 2
        self.z = self.tp // 2
        self.core = self.tp % 2
        self.col = self.sp % 2
        self.line = self.sp // 2
        self.across = self.line * 2 + 1 - self.col
        self.along = (1 - self.line) * 2 + self.col
        self.far = (1 - self.line) * 2 + 1 - self.col
        self.partner = (self.sp, self.z * 2 + 1 - self.core)
        self.x_next = (self.across, self.tp)
        self.y_next = (self.along, self.tp)

    def z_peer(self, step):
        return lax.rem(self.z + step, self.depth)

    def z_device(self, step):
        return (self.sp, self.z_peer(step) * 2 + self.core)

    def meet(self, wide):
        barrier = pltpu.get_barrier_semaphore()
        peers = [self.partner] + [self.z_device(step) for step in range(1, self.depth)]
        if wide:
            peers = peers + [self.x_next, self.y_next]
        for peer in peers:
            pl.semaphore_signal(
                barrier, inc=1, device_id=peer, device_id_type=pl.DeviceIdType.MESH
            )
        pl.semaphore_wait(barrier, len(peers))


def remote(source, target, send_sem, recv_sem, device):
    return pltpu.make_async_remote_copy(
        src_ref=source,
        dst_ref=target,
        send_sem=send_sem,
        recv_sem=recv_sem,
        device_id=device,
        device_id_type=pl.DeviceIdType.MESH,
    )


def add_into(target, first, *others):
    def one(z, nothing):
        total = first[z].astype(jnp.float32)
        for other in others:
            total = total + other[z].astype(jnp.float32)
        target[z] = total.astype(target.dtype)
        return nothing

    lax.fori_loop(0, target.shape[0], one, 0)


def finish_over_z(place, mine, z_recv, send_sems, recv_sems, base_ref, out_ref):
    copies = []
    order = [1] + list(range(place.depth - 1, 1, -1))
    for step in order:
        copy = remote(
            mine.at[place.z_peer(step)],
            z_recv.at[step - 1],
            send_sems.at[step - 1],
            recv_sems.at[step - 1],
            place.z_device(step),
        )
        copy.start()
        copies.append(copy)
    total = mine[place.z].astype(jnp.float32)
    for step, copy in zip(order, copies):
        copy.wait_recv()
        total = total + z_recv[step - 1].astype(jnp.float32)
    out_ref[...] = (base_ref[...].astype(jnp.float32) + total).astype(out_ref.dtype)
    for copy in copies:
        copy.wait_send()


def narrow_kernel(
    parts_ref, base_ref, out_ref, pair_recv, mine, z_recv, pair_send, pair_got, z_send, z_got
):
    place = Places()
    place.meet(False)
    copy = remote(
        parts_ref.at[1 - place.core], pair_recv, pair_send.at[0], pair_got.at[0], place.partner
    )
    copy.start()
    copy.wait_recv()
    add_into(mine, parts_ref.at[place.core], pair_recv)
    finish_over_z(place, mine, z_recv, z_send, z_got, base_ref, out_ref)
    copy.wait_send()


def scatter_sum(parts, base, out_dtype):
    rows, width = base.shape
    depth = lax.axis_size("tp") // 2
    vmem = pl.BlockSpec(memory_space=pltpu.VMEM)

    def room(*lead):
        return pltpu.VMEM(lead + (rows, width), jnp.bfloat16)

    def sems(count):
        return pltpu.SemaphoreType.DMA((count,))

    shaped = parts.reshape(depth, 2, rows, width).transpose(1, 0, 2, 3)
    return pl.pallas_call(
        narrow_kernel,
        out_shape=jax.ShapeDtypeStruct((rows, width), out_dtype),
        in_specs=[vmem] * 2,
        out_specs=vmem,
        scratch_shapes=[room(depth), room(depth), room(depth - 1)]
        + [sems(1), sems(1), sems(depth - 1), sems(depth - 1)],
        compiler_params=pltpu.CompilerParams(
            collective_id=0, has_side_effects=True, vmem_limit_bytes=60 * 2**20
        ),
    )(shaped, base)


class Sends:
    def __init__(self, sems):
        self.sems = sems
        self.made = []

    def start(self, source, target, recv_sem, device, when=None):
        copy = remote(source, target, self.sems.at[len(self.made)], recv_sem, device)
        self.made.append((copy, when))
        if when is None:
            copy.start()
        else:
            pl.when(when)(copy.start)

    def finish(self):
        for copy, when in self.made:
            if when is None:
                copy.wait_send()
            else:
                pl.when(when)(copy.wait_send)


def plane_order(z, depth, step):
    near = jnp.minimum(z, depth - 1 - z)
    if step % 2 == 1:
        swing = z - (step + 1) // 2
    else:
        swing = z + step // 2
    rest = jnp.where(z == near, step, depth - 1 - step)
    return jnp.where(step <= 2 * near, swing, rest)


def layer_kernel(names, head_size, *refs):
    at = types.SimpleNamespace(**dict(zip(names, refs)), head_size=head_size)
    place = Places()
    depth, core, own_z = place.depth, place.core, place.z
    rows, width = at.out.shape
    count = 8 * rows
    half = width // 2
    hidden_width = at.hidden.shape[1]
    tile = 128
    sends = Sends(at.send_sems)
    planes = [plane_order(own_z, depth, step) for step in range(depth)]

    def wait_for(target, sem):
        remote(target, target, at.send_sems.at[0], sem, place.partner).wait_recv()

    attention_copies = []
    pieces = []
    for group in range(at.pack.shape[1]):
        cols = pl.ds(group * 128, 128)
        pieces.append((at.keys.at[:, cols], at.pack.at[place.sp, group, 0]))
        pieces.append((at.values.at[:, cols], at.pack.at[place.sp, group, 1]))
    for index, (source, target) in enumerate(
        pieces
        + [
            (at.queries, at.query_buf),
            (at.out_weight, at.out_w),
            (at.residual, at.base),
        ]
    ):
        copy = pltpu.make_async_copy(source, target, at.copy_sems.at[index])
        copy.start()
        attention_copies.append(copy)
    expert_copies = []
    for index in range(hidden_width // tile):
        for which, source in enumerate((at.gate, at.up)):
            expert_copies.append(
                pltpu.make_async_copy(
                    source.at[:, pl.ds(index * tile, tile)],
                    at.pair_w.at[:, pl.ds((2 * index + which) * tile, tile)],
                    at.weight_sems.at[len(expert_copies)],
                )
            )
    expert_copies.append(
        pltpu.make_async_copy(at.down, at.down_w, at.weight_sems.at[len(expert_copies)])
    )
    for copy in expert_copies:
        copy.start()
    place.meet(True)
    attention_stage(at, place, sends, wait_for, attention_copies)
    share_stage(at, place, sends, wait_for, planes)
    expert_stage(at, place, sends, wait_for, planes, expert_copies)
    sends.finish()


def down_rows(row, rows):
    lanes = row.shape[1]
    row_at = lax.broadcasted_iota(jnp.int32, (rows, lanes), 0)
    lane_at = lax.broadcasted_iota(jnp.int32, (rows, lanes), 1)
    return jnp.sum(jnp.where(row_at == lane_at, row, 0.0), axis=1, keepdims=True)


def attention_stage(at, place, sends, wait_for, copies):
    pack, biases, routes = at.pack, at.biases, at.routes
    groups, seq, lanes = pack.shape[1], pack.shape[3], pack.shape[4]
    size = at.head_size
    heads = groups * lanes // size
    own = place.sp

    def piece(block, group):
        return pack.at[block, group]

    for group in range(groups):
        copies[2 * group].wait()
        copies[2 * group + 1].wait()
        source = piece(own, group)
        sends.start(source, source, at.pack_x.at[own, group], place.x_next)
        sends.start(source, source, at.pack_y.at[own, group], place.y_next)
    biases[own, :heads, :] = at.key_bias[...].astype(jnp.float32)
    choice, amount = at.choice[...], at.amount[...]
    rows = choice.shape[1]
    routes[place.z, place.core, own] = jnp.zeros((8, lanes), jnp.float32)
    for expert in range(4):
        chosen = jnp.where(choice == expert, amount, 0.0)
        total = jnp.sum(chosen, axis=0, keepdims=True)
        routes[place.z, place.core, own, expert : expert + 1, :rows] = total
    mine = routes.at[place.z, place.core, own]
    for target, sem in ((biases.at[own], 0), (mine, 1)):
        sends.start(target, target, at.small_x.at[own, sem], place.x_next)
        sends.start(target, target, at.small_y.at[own, sem], place.y_next)
    row_at = lax.broadcasted_iota(jnp.int32, (seq, seq), 0)
    col_at = lax.broadcasted_iota(jnp.int32, (seq, seq), 1)
    later = at.later
    later[...] = jnp.where(row_at > col_at, 1.0, 0.0).astype(jnp.bfloat16)
    copies[2 * groups].wait()

    def visit(block, group, diagonal):
        attend(
            at.query_buf,
            lambda cols: pack[block, group, 0],
            lambda cols: pack[block, group, 1],
            lambda head: biases[block, head : head + 1, :],
            later,
            at.part.at[block],
            at.total.at[block],
            size,
            diagonal,
            group,
        )

    def earlier(block, group):
        @pl.when(block < own)
        def run():
            visit(block, group, False)

    across, along, far = place.across, place.along, place.far
    for group in range(groups):
        visit(own, group, True)
    for group in range(groups):
        from_x, from_y = piece(across, group), piece(along, group)
        wait_for(from_x, at.pack_x.at[across, group])
        if group < groups // 2:
            sends.start(from_x, from_x, at.pack_far.at[group], place.y_next)
        wait_for(from_y, at.pack_y.at[along, group])
        if group >= groups // 2:
            sends.start(from_y, from_y, at.pack_far.at[group], place.x_next)
        if group == 0:
            for target, sem in ((biases, 0), (routes.at[place.z, place.core], 1)):
                wait_for(target.at[across], at.small_x.at[across, sem])
                wait_for(target.at[along], at.small_y.at[along, sem])
                sends.start(
                    target.at[across], target.at[across], at.small_far.at[sem], place.y_next
                )
        earlier(across, group)
        earlier(along, group)
    for sem, target in enumerate((biases, routes.at[place.z, place.core])):
        wait_for(target.at[far], at.small_far.at[sem])
    mine = routes.at[place.z, place.core]
    sends.start(mine, mine, at.route_side.at[place.z], place.partner)
    for shift in range(1, place.depth):
        sends.start(mine, mine, at.route_z.at[place.z], place.z_device(shift))
    for group in range(groups):
        wait_for(piece(far, group), at.pack_far.at[group])
        earlier(far, group)
    for shift in range(1, place.depth):
        other = place.z_peer(shift)
        got = routes.at[other, place.core]
        wait_for(got, at.route_z.at[other])
        sends.start(got, got, at.route_side.at[other], place.partner)
    part, total = at.part, at.total

    def join(step, nothing):
        block = own - 1 - step
        part[own] = part[own] + jnp.exp(total[own]) * part[block]
        total[own] = total[own] + total[block]
        return nothing

    lax.fori_loop(0, own, join, 0)
    lane_head = lax.broadcasted_iota(jnp.int32, (1, lanes), 1) // size
    for group in range(groups):
        cols = slice(group * lanes, (group + 1) * lanes)
        mixture = part[own, :, cols]
        squares = mixture * mixture
        scaled = mixture
        for inner in range(lanes // size):
            chosen = lane_head == inner
            mean = jnp.sum(jnp.where(chosen, squares, 0.0), axis=1, keepdims=True) / size
            scaled = jnp.where(chosen, mixture * lax.rsqrt(mean + epsilon), scaled)
        first = group * (lanes // size)
        gains = [at.head_gain[first + inner : first + inner + 1, :] for inner in range(lanes // size)]
        gain = jnp.concatenate(gains, axis=1)
        at.attended[:, cols] = (scaled * gain).astype(jnp.bfloat16)
    copies[-2].wait()
    copies[-1].wait()


def share_stage(at, place, sends, wait_for, planes):
    rows, width = at.out.shape
    depth, core = place.depth, place.core
    shares, pair, z_recv = at.shares, at.share_pair, at.share_z
    tile = 512
    for start in range(0, width, tile):
        cols = slice(start, start + tile)
        share = jnp.dot(
            at.attended[...], at.out_w[:, cols], preferred_element_type=jnp.float32
        ).astype(jnp.bfloat16)
        for z in range(depth):
            for side in range(2):
                low = (2 * z + side) * rows
                shares[side, z, :, cols] = share[low : low + rows]
    order = planes[1:][::-1] + planes[:1]
    for plane in order:
        sends.start(
            shares.at[1 - core, plane], pair.at[plane], at.share_side.at[plane], place.partner
        )
    for index, plane in enumerate(order):
        wait_for(pair.at[plane], at.share_side.at[plane])
        total = shares[core, plane].astype(jnp.float32) + pair[plane].astype(jnp.float32)
        if index < depth - 1:
            shares[core, plane] = total.astype(jnp.bfloat16)
            sends.start(
                shares.at[core, plane],
                z_recv.at[place.z],
                at.share_got.at[place.z],
                (place.sp, plane * 2 + core),
            )
    total = total + at.base[...].astype(jnp.float32)
    for plane in planes[1:]:
        wait_for(z_recv.at[plane], at.share_got.at[plane])
        total = total + z_recv[plane].astype(jnp.float32)
    stream = total.astype(jnp.bfloat16)
    at.stream[...] = stream
    normed = rms_scaled(stream.astype(jnp.float32)) * at.norm_gain[...]
    at.normed[...] = normed.astype(jnp.bfloat16)
    for plane in planes:
        side = at.routes.at[plane, 1 - core]
        wait_for(side, at.route_side.at[plane])


def expert_stage(at, place, sends, wait_for, planes, copies):
    depth, core, own_z = place.depth, place.core, place.z
    out_ref, own_ref, stream_ref = at.out, at.normed, at.stream
    rows_buf, pair_w, down_w, hidden = at.rows_buf, at.pair_w, at.down_w, at.hidden
    parts, pair_recv, totals, z_recv = at.parts, at.pair_recv, at.totals, at.z_recv
    x_far, y_far, x_near, y_near = at.x_far, at.y_far, at.x_near, at.y_near
    x_last, y_last, routes = at.x_last, at.y_last, at.routes
    local_sem, z_got, x_got, y_got = at.local_sem, at.z_got, at.x_got, at.y_got
    far_got, side_got, pair_got = at.far_got, at.side_got, at.pair_got
    cross_got, z_sum_got = at.cross_got, at.z_sum_got
    rows, width = out_ref.shape
    count = 8 * rows
    half = width // 2
    hidden_width = hidden.shape[1]
    tile = 128
    main = width - width // 8
    slim = pl.ds(main, width - main)

    def first_part(step):
        return pl.ds(0, half if step == 0 else main // 2)

    def second_part(step):
        return pl.ds(half, half) if step == 0 else pl.ds(main // 2, main // 2)

    def body_part(step):
        return pl.ds(0, width if step == 0 else main)

    left, right = pl.ds(0, half), pl.ds(half, half)
    z_up = (place.sp, (own_z + 1) * 2 + core)
    z_down = (place.sp, (own_z - 1) * 2 + core)
    has_up, has_down = own_z < depth - 1, own_z > 0

    def slot(step, seq):
        return rows_buf.at[planes[step], core, seq]

    inner = jnp.logical_and(has_up, has_down)
    outer = jnp.logical_not(inner)

    def both_of(first, second):
        return first if second is None else jnp.logical_and(first, second)

    def to_partner(step, seq):
        target = slot(step, seq).at[:, body_part(step)]
        sends.start(target, target, side_got.at[planes[step], seq], place.partner)

    def own(step, when=None):
        plane = planes[step]
        target = slot(step, place.sp)
        source, go_up, go_down = own_ref, has_up, has_down
        if step > 0:
            source = target
            go_up = jnp.logical_and(has_up, plane < own_z)
            go_down = jnp.logical_and(has_down, plane > own_z)
            if when is None:
                wait_for(target, z_got.at[plane])
            else:
                pl.when(when)(lambda: wait_for(target, z_got.at[plane]))
        sends.start(source, target, z_got.at[plane], z_up, both_of(go_up, when))
        sends.start(source, target, z_got.at[plane], z_down, both_of(go_down, when))
        part = body_part(step)
        near, there = source.at[:, part], target.at[:, part]
        sends.start(near, there, x_got.at[plane], place.x_next, when)
        sends.start(near, there, y_got.at[plane], place.y_next, when)
        sends.start(source, target, side_got.at[plane, place.sp], place.partner, when)

    def slim_out(seq):
        piece = slot(0, seq).at[:, slim]
        for plane in planes[1:]:
            device = (place.sp, plane * 2 + core)
            sends.start(piece, piece, at.slim_got.at[own_z, seq], device)

    def relay(step):
        plane = planes[step]
        across, along = slot(step, place.across), slot(step, place.along)
        front, back = first_part(step), second_part(step)
        part = body_part(step)
        wait_for(across.at[:, part], x_got.at[plane])
        sends.start(across.at[:, front], across.at[:, front], far_got.at[plane, 0], place.y_next)
        wait_for(along.at[:, part], y_got.at[plane])
        sends.start(along.at[:, back], along.at[:, back], far_got.at[plane, 1], place.x_next)
        to_partner(step, place.across)
        to_partner(step, place.along)
        if step == 0:
            slim_out(place.across)
            slim_out(place.along)

    def far(step):
        plane = planes[step]
        target = slot(step, place.far)
        wait_for(target.at[:, first_part(step)], far_got.at[plane, 0])
        wait_for(target.at[:, second_part(step)], far_got.at[plane, 1])
        to_partner(step, place.far)
        if step == 0:
            slim_out(place.far)

    def slims(step):
        plane = planes[step]
        for seq in (place.across, place.along, place.far):
            piece = slot(step, seq).at[:, slim]
            wait_for(piece, at.slim_got.at[plane, seq])
            sends.start(piece, piece, at.slim_side.at[plane, seq], place.partner)

    def ready(step):
        plane = planes[step]
        for seq in (place.sp, place.across, place.along, place.far):
            target = rows_buf.at[plane, 1 - core, seq]
            if step == 0:
                wait_for(target, side_got.at[plane, seq])
        if step > 0:
            wait_for(rows_buf.at[plane, 1 - core, place.sp], side_got.at[plane, place.sp])
            for seq in (place.across, place.along, place.far):
                target = rows_buf.at[plane, 1 - core, seq]
                wait_for(target.at[:, body_part(step)], side_got.at[plane, seq])
                wait_for(target.at[:, slim], at.slim_side.at[plane, seq])

    def open_tiles(step, low, high):
        plane = planes[step]
        pieces = []
        for side in range(2):
            for seq in range(4):
                row = routes[plane, side, seq, pl.ds(place.sp, 1), :]
                pieces.append(down_rows(row, rows))
        weight = jnp.concatenate(pieces, axis=0)
        block = rows_buf[plane].reshape(count, width)
        for index in range(low, high):
            both = jnp.dot(
                block,
                pair_w[:, 2 * index * tile : 2 * (index + 1) * tile],
                preferred_element_type=jnp.float32,
            )
            gate_part, up_part = both[:, :tile], both[:, tile:]
            value = gate_part / (1.0 + jnp.exp(-gate_part)) * up_part
            value = jnp.where(weight > 0.0, weight * value, 0.0)
            hidden[:, index * tile : (index + 1) * tile] = value.astype(jnp.bfloat16)

    def down_half(step, side):
        spot = right if side else left
        share = jnp.dot(hidden[...], down_w[:, spot], preferred_element_type=jnp.float32)
        parts[step, :, :, :, spot] = share.astype(jnp.bfloat16).reshape(2, 4, rows, half)
        sends.start(
            parts.at[step, 1 - core, :, :, spot],
            pair_recv.at[step, :, :, spot],
            pair_got.at[step, side],
            place.partner,
        )

    def pair_sum(step):
        for side, spot in enumerate((left, right)):
            wait_for(pair_recv.at[step, :, :, spot], pair_got.at[step, side])
        add_into(parts.at[step, core], parts.at[step, core], pair_recv.at[step])

    def first_sends(step):
        mine = parts.at[step, core]
        got = cross_got.at[step]
        sends.start(mine.at[place.far, :, left], x_far.at[step], got.at[0], place.x_next)
        sends.start(mine.at[place.far, :, right], y_far.at[step], got.at[1], place.y_next)
        sends.start(mine.at[place.across, :, left], x_near.at[step], got.at[2], place.x_next)
        sends.start(mine.at[place.along, :, right], y_near.at[step], got.at[3], place.y_next)

    def plus(target, *others):
        total = target.astype(jnp.float32)
        for other in others:
            total = total + other.astype(jnp.float32)
        return total

    def second_sum(step):
        got = cross_got.at[step]
        wait_for(x_far.at[step], got.at[0])
        x_far[step] = plus(x_far[step], parts[step, core, place.along, :, left]).astype(jnp.bfloat16)
        sends.start(x_far.at[step], y_last.at[step], got.at[4], place.y_next)
        wait_for(y_far.at[step], got.at[1])
        y_far[step] = plus(y_far[step], parts[step, core, place.across, :, right]).astype(jnp.bfloat16)
        sends.start(y_far.at[step], x_last.at[step], got.at[5], place.x_next)

    def third_sum(step):
        got = cross_got.at[step]
        wait_for(x_near.at[step], got.at[2])
        wait_for(y_last.at[step], got.at[4])
        low = plus(parts[step, core, place.sp, :, left], x_near[step], y_last[step])
        wait_for(y_near.at[step], got.at[3])
        wait_for(x_last.at[step], got.at[5])
        high = plus(parts[step, core, place.sp, :, right], y_near[step], x_last[step])
        if step > 0:
            totals[step, :, left] = low.astype(jnp.bfloat16)
            totals[step, :, right] = high.astype(jnp.bfloat16)
            sends.start(
                totals.at[step],
                z_recv.at[own_z],
                z_sum_got.at[own_z],
                (place.sp, planes[step] * 2 + core),
            )
        else:
            for shift in range(1, depth):
                other = place.z_peer(shift)
                wait_for(z_recv.at[other], z_sum_got.at[other])
                low = plus(low, z_recv[other, :, left])
                high = plus(high, z_recv[other, :, right])
            out_ref[:, left] = plus(low, stream_ref[:, left]).astype(jnp.bfloat16)
            out_ref[:, right] = plus(high, stream_ref[:, right]).astype(jnp.bfloat16)

    local = pltpu.make_async_copy(own_ref, slot(0, place.sp), local_sem)
    local.start()
    tiles = hidden_width // tile
    some = (tiles + 1) // 2
    own(0)
    own(1)
    relay(0)
    own(2)
    far(0)
    relay(1)
    for copy in copies:
        copy.wait()
    local.wait()
    last = depth - 1
    for step in range(depth):
        ready(step)
        open_tiles(step, 0, some)
        if step + 3 <= last:
            own(step + 3, inner)
        if step == 1:
            pair_sum(0)
            first_sends(0)
        if step >= 2:
            pair_sum(step - 1)
            first_sends(step - 1)
        open_tiles(step, some, tiles)
        if step >= 1 and step + 2 <= last:
            relay(step + 2)
        if step >= 3:
            third_sum(step - 2)
        down_half(step, 0)
        if step == 0:
            down_half(step, 1)
            for later in range(3, depth):
                own(later, outer)
            relay(2)
        if step < last:
            far(step + 1)
        if step > 0:
            down_half(step, 1)
        if step < last:
            slims(step + 1)
        if step >= 2:
            if step == 2:
                second_sum(0)
            second_sum(step - 1)
    pair_sum(last)
    first_sends(last)
    third_sum(last - 1)
    second_sum(last)
    third_sum(last)
    third_sum(0)


def layer(arrays, held, head_size):
    at = types.SimpleNamespace(**arrays)
    rows, width = at.residual.shape
    seq, part_width = at.queries.shape
    hidden_width = at.gate.shape[1]
    depth = lax.axis_size("tp") // 2
    groups = part_width // 128
    vmem = pl.BlockSpec(memory_space=pltpu.VMEM)
    anywhere = pl.BlockSpec(memory_space=pl.ANY)

    def room(*shape):
        return pltpu.VMEM(shape, jnp.bfloat16)

    def wide_room(*shape):
        return pltpu.VMEM(shape, jnp.float32)

    def sems(*shape):
        return pltpu.SemaphoreType.DMA(shape)

    half = room(depth, rows, width // 2)
    total_sends = 48 * depth + 3 * groups + 16
    scratch = dict(
        pack=room(4, groups, 2, seq, 128),
        query_buf=room(seq, part_width),
        out_w=room(part_width, width),
        base=room(rows, width),
        biases=wide_room(4, 8, seq),
        routes=wide_room(depth, 2, 4, 8, 128),
        later=room(seq, seq),
        part=wide_room(4, seq, part_width),
        total=wide_room(4, seq, part_width),
        attended=room(seq, part_width),
        shares=room(2, depth, rows, width),
        share_pair=room(depth, rows, width),
        share_z=room(depth, rows, width),
        stream=room(rows, width),
        normed=room(rows, width),
        rows_buf=room(depth, 2, 4, rows, width),
        pair_w=room(width, 2 * hidden_width),
        down_w=room(hidden_width, width),
        hidden=room(8 * rows, hidden_width),
        parts=room(depth, 2, 4, rows, width),
        pair_recv=room(depth, 4, rows, width),
        x_far=half,
        y_far=half,
        x_near=half,
        y_near=half,
        x_last=half,
        y_last=half,
        totals=room(depth, rows, width),
        z_recv=room(depth, rows, width),
        send_sems=sems(total_sends),
        copy_sems=sems(2 * groups + 3),
        weight_sems=sems(2 * (hidden_width // 128) + 1),
        pack_x=sems(4, groups),
        pack_y=sems(4, groups),
        pack_far=sems(groups),
        small_x=sems(4, 2),
        small_y=sems(4, 2),
        small_far=sems(2),
        route_side=sems(depth),
        route_z=sems(depth),
        share_side=sems(depth),
        share_got=sems(depth),
        local_sem=pltpu.SemaphoreType.DMA,
        z_got=sems(depth),
        x_got=sems(depth),
        y_got=sems(depth),
        far_got=sems(depth, 2),
        side_got=sems(depth, 4),
        slim_got=sems(depth, 4),
        slim_side=sems(depth, 4),
        pair_got=sems(depth, 2),
        cross_got=sems(depth, 6),
        z_sum_got=sems(depth),
    )
    names = list(arrays) + ["out"] + list(scratch)

    def body(*refs):
        layer_kernel(names, head_size, *refs)

    return pl.pallas_call(
        body,
        out_shape=jax.ShapeDtypeStruct((rows, width), jnp.bfloat16),
        in_specs=[anywhere] * held + [vmem] * (len(arrays) - held),
        out_specs=vmem,
        scratch_shapes=list(scratch.values()),
        compiler_params=pltpu.CompilerParams(
            collective_id=1, has_side_effects=True, vmem_limit_bytes=60 * 2**20
        ),
    )(*arrays.values())


def on_device(
    queries,
    keys,
    values,
    key_bias,
    head_gain,
    out_weight,
    residual,
    norm_gain,
    gate_proj,
    up_proj,
    down_proj,
    expert_choice,
    expert_weights,
):
    rows_own = queries.shape[0]
    model_width = out_weight.shape[1]
    seq_devices = lax.axis_size("sp")
    head_devices = lax.axis_size("tp")
    row_share = rows_own // head_devices
    local_experts = gate_proj.shape[0]
    experts_all = local_experts * seq_devices
    capacity = 4 * rows_own // (head_devices * experts_all)
    dense = capacity >= row_share and seq_devices == 4 and head_devices % 4 == 0
    dense = dense and local_experts == 1 and head_devices >= 8 and experts_all == 4
    dense = dense and rows_own % 128 == 0 and row_share <= 128 and queries.shape[1] % 256 == 0
    if dense:
        arrays = dict(
            keys=keys,
            values=values,
            queries=queries,
            out_weight=out_weight,
            residual=residual,
            gate=gate_proj[0],
            up=up_proj[0],
            down=down_proj[0],
            key_bias=key_bias.T,
            head_gain=head_gain,
            norm_gain=norm_gain.reshape(1, -1),
            choice=expert_choice.T,
            amount=expert_weights.T,
        )
        return layer(arrays, 8, head_gain.shape[1])
    attended = attention(queries, keys, values, key_bias, head_gain)
    shares = jnp.dot(attended, out_weight, preferred_element_type=jnp.float32)
    stream = scatter_sum(shares.astype(jnp.bfloat16), residual, jnp.bfloat16)
    normed = (rms_scaled(stream.astype(jnp.float32)) * norm_gain).astype(jnp.bfloat16)
    own_slots = expert_choice * capacity + choice_ranks(expert_choice, experts_all)
    wanted = slot_tokens(own_slots, experts_all * capacity, row_share)
    outgoing = jnp.take(normed, wanted, axis=0, mode="fill", fill_value=0)
    arrived = lax.all_to_all(
        outgoing.reshape(seq_devices, local_experts, capacity, model_width),
        "sp",
        split_axis=0,
        concat_axis=0,
        tiled=True,
    )
    row_piece = lax.all_gather(arrived, "tp", axis=0, tiled=True)
    count_rows = row_piece.shape[0]
    partials = jnp.stack(
        [
            expert_partial(
                row_piece[:, 0].reshape(-1, model_width), gate_proj[0], up_proj[0], down_proj[0]
            ).reshape(count_rows, capacity, model_width)
        ],
        axis=1,
    )
    summed = lax.psum_scatter(partials.astype(jnp.bfloat16), "tp", scatter_dimension=0, tiled=True)
    returned = lax.all_to_all(summed, "sp", split_axis=0, concat_axis=0, tiled=True).reshape(
        experts_all * capacity, model_width
    )
    picked = jnp.take(returned, own_slots, axis=0).astype(jnp.float32)
    combined = jnp.sum(expert_weights[:, :, None] * picked, axis=1)
    return (stream.astype(jnp.float32) + combined).astype(jnp.bfloat16)


def solution(mesh):
    placed = (
        P("sp", "tp"),
        P("sp", "tp"),
        P("sp", "tp"),
        P("sp", "tp"),
        P("tp", None),
        P("tp", None),
        P(("sp", "tp"), None),
        P(),
        P("sp", None, "tp"),
        P("sp", None, "tp"),
        P("sp", "tp", None),
        P(("sp", "tp"), None),
        P(("sp", "tp"), None),
    )
    return jax.shard_map(
        on_device, mesh=mesh, in_specs=placed, out_specs=P(("sp", "tp"), None), check_vma=False
    )
```
